32 devices in a mesh: sp: 8 (over z, x), tp: 4 (over y, core).
Axes of the slice: x: 2, y: 2, z: 4, core: 2. Of those that a mesh axis runs over, the one named last changes fastest.
Arguments:
- cotangent: bfloat16 [1024, 2048], P('sp'), may hold values from -6 to 6
- stream: bfloat16 [1024, 2048], P('sp'), may hold values from -6 to 6
- routes: int32 [1024, 2], P('sp'), may hold values from 0 to 3, all different within a row; in each aligned block of 128 rows (0 to 127, 128 to 255, ...) at most 96 rows name the same one
- route_weights: float32 [1024, 2], P('sp'), may hold values from 0.25 to 1
- gate_weight: bfloat16 [8, 2048, 2048], P('sp', None, 'tp'), may hold values from -0.125 to 0.125
- up_weight: bfloat16 [8, 2048, 2048], P('sp', None, 'tp'), may hold values from -0.125 to 0.125
- down_weight: bfloat16 [8, 2048, 2048], P('sp', 'tp'), may hold values from -0.09375 to 0.09375
- outer_gate: bfloat16 [1024, 1024], P('sp', 'tp'), may hold values from -6 to 6
- inner_gate: bfloat16 [1024, 1024], P('sp', 'tp'), may hold values from -6 to 6
- conv_input: bfloat16 [1024, 1024], P('sp', 'tp'), may hold values from -6 to 6
- conv_taps: bfloat16 [3, 1024], P(None, 'tp'), may hold values from -1 to 1
- out_weight: bfloat16 [2048, 1024], P(None, 'tp'), may hold values from -0.1875 to 0.1875
Outputs:
- gate_grad: bfloat16 [8, 2048, 2048], P('sp', None, 'tp')
- up_grad: bfloat16 [8, 2048, 2048], P('sp', None, 'tp')
- down_grad: bfloat16 [8, 2048, 2048], P('sp', 'tp')
- out_grad: float32 [2048, 1024], P('sp', 'tp')
- outer_grad: bfloat16 [1024, 1024], P('sp', 'tp')
- inner_grad: bfloat16 [1024, 1024], P('sp', 'tp')
- input_grad: bfloat16 [1024, 1024], P('sp', 'tp')
The draws below stay inside these ranges and needn't reach their ends.
Inputs may be any that keep to these rules, and one draw needn't show every extreme that they name: `routes`: each token names two different experts. Among the 128 tokens of one index of sp no expert is named by more than 96 tokens, a bound that some block of them reaches in every draw.
All inputs are finite; a program needn't handle non-finite values.
Results may differ from the reference program's by a relative error of at most 0.02.
Values may be sent and summed in bfloat16 or wider, within the bound.
A program may use at most 64 MiB of HBM per device.

```python
import math
import jax
import jax.numpy as jnp
import numpy as np
from jax import lax

D = 2048
HID = 4096
CONV = 1024
TOK_DEV = 128
HALF = 2048
CAP = 96
TOKENS = 1024
N_SP = 8
N_TP = 4


def with_spikes(entries, own_key, source, target, shards_of, factor):
    def block_of(axis_at):
        return (jnp.arange(entries.shape[axis_at]) // (entries.shape[axis_at] // shards_of)).reshape((-1,) + (1,) * (entries.ndim - 1 - axis_at))

    near = jax.random.permutation(own_key, shards_of)[block_of(target)]
    far = (block_of(target) + shards_of // 2) % shards_of
    return jnp.where((block_of(source) == near) | (block_of(source) == far), factor * entries, entries)


def block_levels(key, extent, cuts, smallest, largest):
    def one(position, parts):
        steps = jax.random.uniform(jax.random.fold_in(jax.random.fold_in(key, 6), position), (parts,), jnp.float32, smallest / len(cuts), largest / len(cuts))
        return jnp.repeat(jnp.exp(steps), extent[position] // parts).reshape((-1,) + (1,) * (len(extent) - position - 1))

    loudness = one(*cuts[0])
    for cut in cuts[1:]:
        loudness = loudness * one(*cut)
    return loudness


def routed_block(key, own, number, rows, number_of, top, most, skew):
    ranking = jax.random.permutation(key, number_of)
    crowded, ordinary = portions_of(number_of, rows * top, most, skew, True), portions_of(number_of, rows * top, most, skew, False)
    places = jnp.arange(number_of)

    def named(sizes, rotation):
        used = int((sizes > 0).sum())
        fixed = max(1, used // 4)
        shifted = fixed + (places - fixed + rotation * (used - fixed)) % max(1, number_of - fixed)
        return jnp.zeros((number_of,), jnp.int32).at[ranking[jnp.where(places < fixed, places, shifted)]].set(jnp.asarray(sizes, jnp.int32))

    sizes = jnp.where(number % 4 == 0, named(crowded, number // 4), named(ordinary, number - number // 4 - 1))
    mixed = jax.random.permutation(jax.random.fold_in(own, 3), number_of)
    donor, sink = mixed[0:number_of // 2 * 2:2], mixed[1:number_of // 2 * 2:2]
    margin = jnp.minimum(sizes[donor] - 1, most - sizes[sink]) // 2
    margin = jnp.where((donor == ranking[0]) | (sink == ranking[0]) | (sizes[sink] == 0), 0, jnp.maximum(margin, 0))
    shifted = jax.random.randint(jax.random.fold_in(own, 4), (number_of // 2,), 0, 1 << 20) % (margin + 1)
    sizes = sizes.at[donor].add(-shifted).at[sink].add(shifted)
    items = jnp.searchsorted(jnp.cumsum(sizes), jnp.arange(rows * top), side="right").astype(jnp.int32)
    grid = items.reshape(top, rows).T
    grid = grid[jax.random.permutation(jax.random.fold_in(own, 1), rows)]
    rotation = jax.random.randint(jax.random.fold_in(own, 2), (rows, 1), 0, top)
    return jnp.take_along_axis(grid, (jnp.arange(top)[None, :] + rotation) % top, axis=1)


def portions_of(count, total, reach, skew, full):
    weights = [(1 << 20) // math.isqrt(rank ** skew) + 1 for rank in range(1, count + 1)]
    largest = reach if full else min(reach, max(-(-total // count), total * weights[0] // sum(weights)))
    least = 1 if total - largest >= count - 1 else 0
    given, rest = [largest] + [least] * (count - 1), total - largest - least * (count - 1)
    while rest > 0:
        movable = [i for i in range(1, count) if given[i] < largest] or [i for i in range(1, count) if given[i] < reach]
        mass, left = sum([weights[i] for i in movable]), rest
        for i in movable:
            extra = min(reach - given[i], max(1, left * weights[i] // mass), rest)
            given[i] = given[i] + extra
            rest = rest - extra
    return np.array(given)


def scatter_about(stream_key, extent, spread, most, cuts=(), held_as=jnp.bfloat16):
    result = spread * jax.random.normal(stream_key, extent, jnp.float32)
    if cuts:
        result = result * block_levels(stream_key, extent, cuts, -0.22, 0.18)
    return jnp.clip(result, -most, most).astype(held_as)


def gaussian_with(key, shape, scale, most, pieces, heavy, kind=jnp.bfloat16):
    array = scale * jax.random.normal(key, shape, jnp.float32)
    if pieces:
        array = array * block_levels(key, shape, pieces, -0.22, 0.18)
    return jnp.clip(with_spikes(array, jax.random.fold_in(key, 3), *heavy), -most, most).astype(kind)


def setup_inputs(seed: int = 0) -> dict:
    keys = jax.random.split(jax.random.key(seed), 13)
    cotangent = gaussian_with(keys[0], (TOKENS, D), 1.0, 6.0, ((0, 8),), (0, 1, 8, 2.0))
    stream = scatter_about(keys[1], (TOKENS, D), 1.0, 6.0, ((0, 8),))
    routes_keys = jax.random.split(jax.random.fold_in(keys[2], 1), TOKENS // TOK_DEV)
    routes_turns = jax.random.permutation(jax.random.fold_in(keys[2], 3), TOKENS // TOK_DEV)
    routes = jax.vmap(lambda own, number: routed_block(jax.random.fold_in(keys[2], 2), own, number, TOK_DEV, N_SP // 2, 2, CAP, 1))(routes_keys, routes_turns).reshape((TOKENS, 2))
    route_weights = jnp.clip(0.25 + 0.75 * jax.random.uniform(keys[3], (TOKENS, 2), jnp.float32) ** block_levels(keys[3], (TOKENS, 2), ((0, 8),), -0.2, 0.2), 0.25, 1.0)
    gate_weight = scatter_about(keys[4], (N_SP, D, HALF), D ** -0.5, 0.125, ((0, 8), (2, 4)))
    up_weight = scatter_about(keys[5], (N_SP, D, HALF), D ** -0.5, 0.125, ((0, 8), (2, 4)))
    down_weight = scatter_about(keys[6], (N_SP, HALF, D), HID ** -0.5, 0.09375, ((0, 8), (1, 4)))
    outer_gate = scatter_about(keys[7], (TOKENS, CONV), 1.0, 6.0, ((0, 8), (1, 4)))
    inner_gate = scatter_about(keys[8], (TOKENS, CONV), 1.0, 6.0, ((0, 8), (1, 4)))
    conv_input = scatter_about(keys[9], (TOKENS, CONV), 1.0, 6.0, ((0, 8), (1, 4)))
    conv_taps = jnp.clip(jax.random.uniform(keys[10], (3, CONV), jnp.float32, -1.0, 1.0) * block_levels(keys[10], (3, CONV), ((1, 4),), -0.4, 0.0), -1.0, 1.0).astype(jnp.bfloat16)
    out_weight = scatter_about(keys[11], (D, CONV), CONV ** -0.5, 0.1875, ((1, 4),))
    return {"cotangent": cotangent, "stream": stream, "routes": routes, "route_weights": route_weights, "gate_weight": gate_weight, "up_weight": up_weight, "down_weight": down_weight, "outer_gate": outer_gate, "inner_gate": inner_gate, "conv_input": conv_input, "conv_taps": conv_taps, "out_weight": out_weight}


def reference(cotangent, stream, routes, route_weights, gate_weight, up_weight, down_weight, outer_gate, inner_gate, conv_input, conv_taps, out_weight):
    tok_count = stream.shape[0]
    model_width = stream.shape[1]
    experts = N_SP // 2
    limit = N_SP * CAP
    blocks = N_TP
    block_units = HALF // N_TP
    flat_routes = routes.reshape(-1).astype(jnp.int32)
    flat_weights = route_weights.reshape(-1).astype(jnp.float32)
    flat_tokens = (jnp.arange(2 * tok_count) // 2).astype(jnp.int32)

    def one_expert(moe_sum, index):
        hits = flat_routes == index
        picked = jnp.nonzero(hits, size=limit, fill_value=0)[0].astype(jnp.int32)
        live_mask = jnp.arange(limit) < jnp.sum(hits.astype(jnp.int32))
        tok_index = flat_tokens[picked]
        weights = jnp.where(live_mask, flat_weights[picked], jnp.float32(0.0))
        routed_rows = jnp.where(live_mask[:, None], stream[tok_index], jnp.zeros((), jnp.bfloat16))
        routed_cot = (weights[:, None] * cotangent[tok_index].astype(jnp.float32)).astype(jnp.bfloat16)
        gate_pair = lax.dynamic_slice_in_dim(gate_weight, 2 * index, 2, 0)
        up_pair = lax.dynamic_slice_in_dim(up_weight, 2 * index, 2, 0)
        down_pair = lax.dynamic_slice_in_dim(down_weight, 2 * index, 2, 0)
        gate_full = jnp.concatenate([gate_pair[0], gate_pair[1]], axis=1)
        up_full = jnp.concatenate([up_pair[0], up_pair[1]], axis=1)
        down_full = jnp.concatenate([down_pair[0], down_pair[1]], axis=0)
        gate_pre = jnp.dot(routed_rows, gate_full, preferred_element_type=jnp.float32)
        up_pre = jnp.dot(routed_rows, up_full, preferred_element_type=jnp.float32)
        hidden_grad = jnp.dot(routed_cot, down_full.T, preferred_element_type=jnp.float32)
        sigma = jax.nn.sigmoid(gate_pre)
        silu_gate = gate_pre * sigma
        hidden = (silu_gate * up_pre).astype(jnp.bfloat16)
        up_delta = (hidden_grad * silu_gate).astype(jnp.bfloat16)
        gate_delta = (hidden_grad * up_pre * sigma * (1.0 + gate_pre * (1.0 - sigma))).astype(jnp.bfloat16)
        gate_grad = jnp.dot(routed_rows.T, gate_delta, preferred_element_type=jnp.float32).astype(jnp.bfloat16)
        up_grad = jnp.dot(routed_rows.T, up_delta, preferred_element_type=jnp.float32).astype(jnp.bfloat16)
        down_grad = jnp.dot(hidden.T, routed_cot, preferred_element_type=jnp.float32).astype(jnp.bfloat16)
        gate_blocks = gate_delta.astype(jnp.float32).reshape(limit, 2 * blocks, block_units)
        up_blocks = up_delta.astype(jnp.float32).reshape(limit, 2 * blocks, block_units)
        gate_table = gate_full.astype(jnp.float32).reshape(model_width, 2 * blocks, block_units)
        up_table = up_full.astype(jnp.float32).reshape(model_width, 2 * blocks, block_units)
        block_part = jnp.einsum("sgh,dgh->gsd", gate_blocks, gate_table) + jnp.einsum("sgh,dgh->gsd", up_blocks, up_table)
        block_part = lax.optimization_barrier(block_part.astype(jnp.bfloat16)).astype(jnp.float32)
        half_sums = jnp.sum(block_part.reshape(2, blocks, limit, model_width), axis=1)
        half_sums = lax.optimization_barrier(half_sums.astype(jnp.bfloat16)).astype(jnp.float32)
        route_sum = jnp.where(live_mask[:, None], half_sums[0] + half_sums[1], jnp.float32(0.0))
        moe_sum = moe_sum.at[tok_index].add(route_sum)
        gate_out = jnp.transpose(gate_grad.reshape(model_width, 2, HALF), (1, 0, 2))
        up_out = jnp.transpose(up_grad.reshape(model_width, 2, HALF), (1, 0, 2))
        down_out = down_grad.reshape(2, HALF, model_width)
        return moe_sum, (gate_out, up_out, down_out)

    moe_sum, stacked = lax.scan(one_expert, jnp.zeros((tok_count, model_width), jnp.float32), jnp.arange(experts, dtype=jnp.int32))
    gate_grad = stacked[0].reshape(N_SP, model_width, HALF)
    up_grad = stacked[1].reshape(N_SP, model_width, HALF)
    down_grad = stacked[2].reshape(N_SP, HALF, model_width)
    moe_grad = moe_sum.astype(jnp.bfloat16)
    stream_grad = (cotangent.astype(jnp.float32) + moe_grad.astype(jnp.float32)).astype(jnp.bfloat16)

    taps = conv_taps.astype(jnp.float32)
    mixed = inner_gate.astype(jnp.float32) * conv_input.astype(jnp.float32)
    padded = jnp.pad(mixed, ((2, 0), (0, 0)))
    conv_sum = taps[0] * padded[:-2] + taps[1] * padded[1:-1] + taps[2] * padded[2:]
    conv_out = (outer_gate.astype(jnp.float32) * conv_sum).astype(jnp.bfloat16)
    out_grad = jnp.dot(stream_grad.T, conv_out, preferred_element_type=jnp.float32)
    conv_grad = jnp.dot(stream_grad, out_weight, preferred_element_type=jnp.float32)
    outer_grad = (conv_grad * conv_sum).astype(jnp.bfloat16)
    scaled = conv_grad * outer_gate.astype(jnp.float32)
    later = jnp.pad(scaled, ((0, 2), (0, 0)))
    mixed_grad = taps[2] * later[:-2] + taps[1] * later[1:-1] + taps[0] * later[2:]
    inner_grad = (mixed_grad * conv_input.astype(jnp.float32)).astype(jnp.bfloat16)
    input_grad = (mixed_grad * inner_gate.astype(jnp.float32)).astype(jnp.bfloat16)
    return (gate_grad, up_grad, down_grad, out_grad, outer_grad, inner_grad, input_grad)
```

```python
import functools

import jax
import jax.numpy as jnp
from jax import lax
from jax.experimental import pallas as pl
from jax.experimental.pallas import tpu as pltpu
from jax.sharding import PartitionSpec as P


def from_behind(block, axis, distance):
    devices = range(lax.axis_size(axis))
    route = [(i - distance, i) for i in devices if i - distance in devices]
    return lax.ppermute(block, axis, route)


def near_first(count):
    return sorted(range(count), key=lambda d: (min(d, count - d), d))


class Seat:
    def __init__(self, experts, pairs):
        self.sp = lax.axis_index("sp")
        self.tp = lax.axis_index("tp")
        self.half = lax.rem(self.sp, 2)
        self.expert = self.sp // 2
        self.core = lax.rem(self.tp, 2)
        self.row = self.tp // 2
        self.experts = experts
        self.pairs = pairs

    def ahead(self, distance):
        return lax.rem(self.expert + distance, self.experts)

    def behind(self, distance):
        return lax.rem(self.expert + self.experts - distance, self.experts)

    def other_expert(self, expert):
        return (expert * 2 + self.half, self.tp)

    def other_half(self):
        return (self.expert * 2 + 1 - self.half, self.tp)

    def row_ahead(self, distance):
        return lax.rem(self.row + distance, self.pairs)

    def row_behind(self, distance):
        return lax.rem(self.row + self.pairs - distance, self.pairs)

    def other_row(self, row):
        return (self.sp, row * 2 + self.core)

    def other_core(self):
        return (self.sp, self.row * 2 + 1 - self.core)


def remote(src, dst, sent, landed, device):
    return pltpu.make_async_remote_copy(
        src_ref=src,
        dst_ref=dst,
        send_sem=sent,
        recv_sem=landed,
        device_id=device,
        device_id_type=pl.DeviceIdType.MESH,
    )


def greet(peers):
    barrier = pltpu.get_barrier_semaphore()
    for peer in peers:
        pl.semaphore_signal(barrier, inc=1, device_id=peer, device_id_type=pl.DeviceIdType.MESH)
    pl.semaphore_wait(barrier, len(peers))


def dispatch_kernel(experts, pairs, send_ref, rows_ref, cot_ref,
                    zs, zr, xs, xr, ys, yr, ds, dr, cs, cr, own):
    seat = Seat(experts, pairs)
    width = send_ref.shape[3]
    offs = near_first(experts)
    outs = (rows_ref, cot_ref)
    greet(
        [seat.other_expert(seat.ahead(d)) for d in range(1, experts)]
        + [seat.other_half(), seat.other_core()]
        + [seat.other_row(seat.row_ahead(d)) for d in range(1, pairs)]
    )
    started = []

    def place(kind, half, expert, tp):
        cols = pl.ds(pl.multiple_of(tp * width, width), width)
        return outs[kind].at[half, expert, :, cols]

    def push(src, dst, sent, landed, device):
        copy = remote(src, dst, sent, landed, device)
        copy.start()
        started.append(copy)

    def landed(spot, sem_s, sem_r):
        remote(spot, spot, sem_s, sem_r, seat.other_core()).wait_recv()

    items = [(kind, k) for kind in range(2) for k in range(experts)]
    local = []
    for kind in range(2):
        spot = place(kind, seat.half, seat.expert, seat.tp)
        copy = pltpu.make_async_copy(send_ref.at[kind, seat.expert], spot, own.at[kind])
        copy.start()
        local.append(copy)
        for k in range(1, experts):
            target = seat.behind(offs[k])
            push(send_ref.at[kind, target], spot, zs.at[kind, k], zr.at[kind, k],
                 seat.other_expert(target))

    def first(kind, k):
        spot = place(kind, seat.half, seat.ahead(offs[k]), seat.tp)
        if k == 0:
            src = send_ref.at[kind, seat.expert]
        else:
            landed(spot, zs.at[kind, k], zr.at[kind, k])
            src = spot
        push(src, spot, xs.at[kind, k], xr.at[kind, k], seat.other_half())
        for d in range(1, pairs):
            push(src, spot, ys.at[kind, k, d], yr.at[kind, k, d],
                 seat.other_row(seat.row_behind(d)))
        push(src, spot, cs.at[kind, k, 0], cr.at[kind, k, 0], seat.other_core())

    def second(kind, k):
        expert = seat.ahead(offs[k])
        spot = place(kind, 1 - seat.half, expert, seat.tp)
        landed(spot, xs.at[kind, k], xr.at[kind, k])
        if k % 2 == 0:
            for d in range(1, pairs):
                push(spot, spot, ds.at[kind, k, d], dr.at[kind, k, d],
                     seat.other_row(seat.row_behind(d)))
        push(spot, spot, cs.at[kind, k, 1], cr.at[kind, k, 1], seat.other_core())
        for d in range(1, pairs):
            spot = place(kind, seat.half, expert, seat.row_ahead(d) * 2 + seat.core)
            landed(spot, ys.at[kind, k, d], yr.at[kind, k, d])
            if k % 2 == 1:
                push(spot, spot, ds.at[kind, k, d], dr.at[kind, k, d], seat.other_half())
            push(spot, spot, cs.at[kind, k, 2 * d], cr.at[kind, k, 2 * d], seat.other_core())

    def third(kind, k):
        for d in range(1, pairs):
            spot = place(kind, 1 - seat.half, seat.ahead(offs[k]),
                         seat.row_ahead(d) * 2 + seat.core)
            landed(spot, ds.at[kind, k, d], dr.at[kind, k, d])
            push(spot, spot, cs.at[kind, k, 2 * d + 1], cr.at[kind, k, 2 * d + 1],
                 seat.other_core())

    for n in range(len(items) + 2):
        if n < len(items):
            first(*items[n])
        if 1 <= n <= len(items):
            second(*items[n - 1])
        if n >= 2:
            third(*items[n - 2])
    for kind, k in items:
        expert = seat.ahead(offs[k])
        for d in range(pairs):
            tp = seat.row_ahead(d) * 2 + 1 - seat.core
            for swap in range(2):
                half = seat.half if swap == 0 else 1 - seat.half
                landed(place(kind, half, expert, tp),
                       cs.at[kind, k, 2 * d + swap], cr.at[kind, k, 2 * d + swap])
    for copy in started:
        copy.wait_send()
    for copy in local:
        copy.wait()


def return_kernel(experts, pairs, part_ref, sel_ref, cot_ref, conv_ref, sg_ref, g_ref, c_ref,
                  a_ref, acc_ref, b1_ref, acc2_ref, b2_ref, fin_ref, ret_ref,
                  as_, ar, b1s, b1r, b2s, b2r, zs, zr, ms, mr, gs, gr, vs, vr, us, ur, own):
    seat = Seat(experts, pairs)
    capacity = part_ref.shape[2]
    width = part_ref.shape[3] // (2 * pairs)
    slice_width = g_ref.shape[3]
    offs = near_first(experts)
    order = list(reversed(range(experts)))
    sp_peers = [
        (expert * 2 + half, seat.tp)
        for d in range(experts)
        for expert in [seat.ahead(d)]
        for half in ([seat.half, 1 - seat.half] if d else [1 - seat.half])
    ]
    greet(
        sp_peers + [seat.other_core()]
        + [seat.other_row(seat.row_ahead(d)) for d in range(1, pairs)]
    )
    started = []

    def cols(tp):
        return pl.ds(pl.multiple_of(tp * width, width), width)

    def push(src, dst, sent, landed, device):
        copy = remote(src, dst, sent, landed, device)
        copy.start()
        started.append(copy)

    def landed(spot, sem_s, sem_r):
        remote(spot, spot, sem_s, sem_r, seat.other_core()).wait_recv()

    def total(*terms):
        value = terms[0].astype(jnp.float32)
        for term in terms[1:]:
            value = value + term.astype(jnp.float32)
        return value.astype(jnp.bfloat16)

    def zone(k):
        return seat.behind(offs[k])

    for k in order:
        for half in range(2):
            for row in range(pairs):
                push(part_ref.at[half, zone(k), :, cols(row * 2 + 1 - seat.core)],
                     a_ref.at[half, row, k], as_.at[half, row, k], ar.at[half, row, k],
                     seat.other_core())
    copy_conv = pltpu.make_async_copy(conv_ref, c_ref.at[seat.half, seat.expert], own.at[0])
    copy_conv.start()
    for k in range(1, experts):
        push(conv_ref, c_ref.at[seat.half, seat.expert], vs.at[k], vr.at[k],
             seat.other_expert(seat.behind(offs[k])))

    def first(k):
        for half in range(2):
            for row in range(pairs):
                landed(a_ref.at[half, row, k], as_.at[half, row, k], ar.at[half, row, k])
                acc_ref[half, row, k] = total(
                    part_ref[half, zone(k), :, cols(row * 2 + seat.core)], a_ref[half, row, k]
                )
        if k % 2 == 0:
            for row in range(pairs):
                push(acc_ref.at[1 - seat.half, row, k], b1_ref.at[k, row],
                     b1s.at[k, row], b1r.at[k, row], seat.other_half())
        else:
            for d in range(1, pairs):
                target = seat.row_behind(d)
                for half in range(2):
                    slot = 2 * (d - 1) + half
                    push(acc_ref.at[half, target, k], b1_ref.at[k, slot],
                         b1s.at[k, slot], b1r.at[k, slot], seat.other_row(target))

    def second(k):
        if k % 2 == 0:
            for row in range(pairs):
                landed(b1_ref.at[k, row], b1s.at[k, row], b1r.at[k, row])
                acc2_ref[k, row] = total(acc_ref[seat.half, row, k], b1_ref[k, row])
            for d in range(1, pairs):
                target = seat.row_behind(d)
                push(acc2_ref.at[k, target], b2_ref.at[k, d - 1], b2s.at[k, d - 1],
                     b2r.at[k, d - 1], seat.other_row(target))
        else:
            for half in range(2):
                terms = [acc_ref[half, seat.row, k]]
                for d in range(1, pairs):
                    slot = 2 * (d - 1) + half
                    landed(b1_ref.at[k, slot], b1s.at[k, slot], b1r.at[k, slot])
                    terms.append(b1_ref[k, slot])
                acc2_ref[k, half] = total(*terms)
            push(acc2_ref.at[k, 1 - seat.half], b2_ref.at[k, 0], b2s.at[k, 0], b2r.at[k, 0],
                 seat.other_half())

    def third(k):
        count = pairs - 1 if k % 2 == 0 else 1
        terms = [acc2_ref[k, seat.row if k % 2 == 0 else seat.half]]
        for slot in range(count):
            landed(b2_ref.at[k, slot], b2s.at[k, slot], b2r.at[k, slot])
            terms.append(b2_ref[k, slot])
        rows = pl.ds(pl.multiple_of(seat.expert * capacity, 16), capacity)
        if k == 0:
            ret_ref[rows, :] = total(*terms)
        else:
            fin_ref[k] = total(*terms)
            push(fin_ref.at[k], ret_ref.at[rows, :], zs.at[k], zr.at[k],
                 seat.other_expert(zone(k)))

    for n in range(experts + 2):
        if n < experts:
            first(order[n])
        if 1 <= n <= experts:
            second(order[n - 1])
        if n >= 2:
            third(order[n - 2])
    copy_conv.wait()
    for k in range(experts):
        expert = seat.ahead(offs[k])
        spot = c_ref.at[seat.half, expert]
        if k:
            landed(spot, vs.at[k], vr.at[k])
        push(spot, spot, us.at[k], ur.at[k], seat.other_half())
    for k in range(1, experts):
        rows = pl.ds(pl.multiple_of(seat.ahead(offs[k]) * capacity, 16), capacity)
        landed(ret_ref.at[rows, :], zs.at[k], zr.at[k])
    moe = jnp.dot(sel_ref[...], ret_ref[...], preferred_element_type=jnp.float32)
    mine = cols(seat.tp)
    sg_ref[:, mine] = total(cot_ref[:, mine], moe.astype(jnp.bfloat16))
    for d in range(1, pairs):
        push(sg_ref.at[:, mine], sg_ref.at[:, mine], ms.at[2 * d], mr.at[2 * d],
             seat.other_row(seat.row_behind(d)))
    push(sg_ref.at[:, mine], sg_ref.at[:, mine], ms.at[0], mr.at[0], seat.other_core())
    for d in range(1, pairs):
        theirs = sg_ref.at[:, cols(seat.row_ahead(d) * 2 + seat.core)]
        landed(theirs, ms.at[2 * d], mr.at[2 * d])
        push(theirs, theirs, ms.at[2 * d + 1], mr.at[2 * d + 1], seat.other_core())
    for d in range(pairs):
        slot = 0 if d == 0 else 2 * d + 1
        theirs = sg_ref.at[:, cols(seat.row_ahead(d) * 2 + 1 - seat.core)]
        landed(theirs, ms.at[slot], mr.at[slot])

    def piece(sp):
        return sg_ref.at[:, pl.ds(pl.multiple_of(sp * slice_width, 128), slice_width)]

    for k in range(experts):
        expert = seat.behind(offs[k])
        for swap in range(2):
            if k == 0 and swap == 0:
                continue
            half = seat.half if swap == 0 else 1 - seat.half
            push(piece(expert * 2 + half), g_ref.at[seat.half, seat.expert],
                 gs.at[k, swap], gr.at[k, swap], (expert * 2 + half, seat.tp))
    keep = pltpu.make_async_copy(piece(seat.sp), g_ref.at[seat.half, seat.expert], own.at[1])
    keep.start()
    for k in range(experts):
        expert = seat.ahead(offs[k])
        landed(c_ref.at[1 - seat.half, expert], us.at[k], ur.at[k])
        for swap in range(2):
            if k == 0 and swap == 0:
                continue
            half = seat.half if swap == 0 else 1 - seat.half
            landed(g_ref.at[half, expert], gs.at[k, swap], gr.at[k, swap])
    for copy in started:
        copy.wait_send()
    keep.wait()


def vmem(count):
    return [pl.BlockSpec(memory_space=pltpu.VMEM)] * count


def sems(*shape):
    return pltpu.SemaphoreType.DMA(shape)


def dispatch(sent, experts, tp_count):
    pairs = tp_count // 2
    _, _, capacity, width = sent.shape
    shape = jax.ShapeDtypeStruct((2, experts, capacity, width * tp_count), jnp.bfloat16)
    flat, rowed = (2, experts), (2, experts, pairs)
    cored = (2, experts, 2 * pairs)
    return pl.pallas_call(
        functools.partial(dispatch_kernel, experts, pairs),
        out_shape=(shape, shape),
        in_specs=vmem(1),
        out_specs=tuple(vmem(2)),
        scratch_shapes=[
            sems(*s)
            for s in (flat, flat, flat, flat, rowed, rowed, rowed, rowed, cored, cored, (2,))
        ],
        compiler_params=pltpu.CompilerParams(
            collective_id=0, has_side_effects=True, vmem_limit_bytes=32 * 1024 * 1024
        ),
    )(sent)


def give_back(part, select_t, cotangent, conv_out, experts, tp_count):
    pairs = tp_count // 2
    _, _, capacity, model_width = part.shape
    tokens, channels = conv_out.shape
    width = model_width // tp_count
    groups = 2 * experts
    most = max(pairs, 2 * (pairs - 1))
    late = max(pairs - 1, 1)
    bf16 = jnp.bfloat16
    return pl.pallas_call(
        functools.partial(return_kernel, experts, pairs),
        out_shape=(
            jax.ShapeDtypeStruct((tokens, model_width), bf16),
            jax.ShapeDtypeStruct((2, experts, tokens, model_width // groups), bf16),
            jax.ShapeDtypeStruct((2, experts, tokens, channels), bf16),
        ),
        in_specs=vmem(4),
        out_specs=tuple(vmem(3)),
        scratch_shapes=[
            pltpu.VMEM((2, pairs, experts, capacity, width), bf16),
            pltpu.VMEM((2, pairs, experts, capacity, width), bf16),
            pltpu.VMEM((experts, most, capacity, width), bf16),
            pltpu.VMEM((experts, max(pairs, 2), capacity, width), bf16),
            pltpu.VMEM((experts, late, capacity, width), bf16),
            pltpu.VMEM((experts, capacity, width), bf16),
            pltpu.VMEM((experts * capacity, width), bf16),
        ]
        + [
            sems(*s)
            for shape in (
                (2, pairs, experts), (experts, most), (experts, late), (experts,),
                (2 * pairs,), (experts, 2), (experts,), (experts,),
            )
            for s in (shape, shape)
        ]
        + [sems(2)],
        compiler_params=pltpu.CompilerParams(
            collective_id=1, has_side_effects=True, vmem_limit_bytes=40 * 1024 * 1024
        ),
    )(part, select_t, cotangent, conv_out)


def per_device(
    cotangent,
    stream,
    routes,
    route_weights,
    gate_weight,
    up_weight,
    down_weight,
    outer_gate,
    inner_gate,
    conv_input,
    conv_taps,
    out_weight,
):
    groups = lax.axis_size("sp")
    tp_count = lax.axis_size("tp")
    experts = groups // 2
    tok_rows = stream.shape[0]
    model_width = stream.shape[1]
    capacity = 3 * tok_rows // experts
    slot_total = experts * capacity
    contract_first = (((0,), (0,)), ((), ()))
    contract_last = (((1,), (1,)), ((), ()))
    flat_routes = routes.reshape(-1)
    choose = (flat_routes[:, None] == jnp.arange(experts, dtype=jnp.int32)[None, :]).astype(
        jnp.int32
    )
    before = jnp.cumsum(choose, axis=0) - choose
    slot_place = flat_routes * capacity + jnp.sum(before * choose, axis=1)
    slot_table = (jnp.arange(slot_total, dtype=jnp.int32)[:, None] == slot_place[None, :]).astype(
        jnp.float32
    )
    select = jnp.sum(slot_table.reshape(slot_total, tok_rows, 2), axis=2).astype(jnp.bfloat16)
    slot_weight = jnp.sum(slot_table * route_weights.reshape(-1)[None, :], axis=1)
    block_width = model_width // tp_count
    offset = lax.axis_index("tp") * block_width
    rows_part = lax.dynamic_slice_in_dim(stream, offset, block_width, 1)
    cot_part = lax.dynamic_slice_in_dim(cotangent, offset, block_width, 1)
    sent_rows = jnp.dot(select, rows_part, preferred_element_type=jnp.float32).astype(jnp.bfloat16)
    sent_cot = (
        jnp.dot(select, cot_part, preferred_element_type=jnp.float32) * slot_weight[:, None]
    ).astype(jnp.bfloat16)
    direct = tp_count % 2 == 0 and capacity % 16 == 0 and block_width % 128 == 0
    slots = groups * capacity
    if direct:
        sent = jnp.stack([sent_rows, sent_cot]).reshape(2, experts, capacity, block_width)
        routed_rows, routed_cot = dispatch(sent, experts, tp_count)
        routed_rows = routed_rows.reshape(slots, model_width)
        routed_cot = routed_cot.reshape(slots, model_width)
    else:
        sent_rows = jnp.repeat(sent_rows.reshape(experts, capacity, -1), 2, axis=0)
        sent_cot = jnp.repeat(sent_cot.reshape(experts, capacity, -1), 2, axis=0)
        recv_rows, recv_cot = (
            lax.all_to_all(sent_rows, "sp", split_axis=0, concat_axis=0, tiled=True),
            lax.all_to_all(sent_cot, "sp", split_axis=0, concat_axis=0, tiled=True),
        )
        recv_rows, recv_cot = (
            lax.all_gather(recv_rows, "tp", axis=2, tiled=True),
            lax.all_gather(recv_cot, "tp", axis=2, tiled=True),
        )
        routed_rows = recv_rows.reshape(slots, model_width)
        routed_cot = recv_cot.reshape(slots, model_width)
    gate_local = gate_weight[0]
    up_local = up_weight[0]
    down_local = down_weight[0]
    gate_pre = jnp.dot(routed_rows, gate_local, preferred_element_type=jnp.float32)
    up_pre = jnp.dot(routed_rows, up_local, preferred_element_type=jnp.float32)
    hidden_grad = lax.dot_general(
        routed_cot, down_local, contract_last, preferred_element_type=jnp.float32
    )
    sigma = jax.nn.sigmoid(gate_pre)
    silu_gate = gate_pre * sigma
    hidden = (silu_gate * up_pre).astype(jnp.bfloat16)
    up_delta = (hidden_grad * silu_gate).astype(jnp.bfloat16)
    gate_delta = (hidden_grad * up_pre * sigma * (1.0 + gate_pre * (1.0 - sigma))).astype(
        jnp.bfloat16
    )
    gate_grad = lax.dot_general(
        routed_rows, gate_delta, contract_first, preferred_element_type=jnp.float32
    ).astype(jnp.bfloat16)[None]
    up_grad = lax.dot_general(
        routed_rows, up_delta, contract_first, preferred_element_type=jnp.float32
    ).astype(jnp.bfloat16)[None]
    down_grad = lax.dot_general(
        hidden, routed_cot, contract_first, preferred_element_type=jnp.float32
    ).astype(jnp.bfloat16)[None]
    row_partial = lax.dot_general(
        gate_delta, gate_local, contract_last, preferred_element_type=jnp.float32
    )
    row_partial = row_partial + lax.dot_general(
        up_delta, up_local, contract_last, preferred_element_type=jnp.float32
    )
    taps = conv_taps.astype(jnp.float32)
    outer_f = outer_gate.astype(jnp.float32)
    inner_f = inner_gate.astype(jnp.float32)
    input_f = conv_input.astype(jnp.float32)
    mixed = inner_f * input_f
    earlier = from_behind(mixed[-2:], "sp", 1)
    padded = jnp.concatenate([earlier, mixed], axis=0)
    conv_sum = taps[0] * padded[:-2] + taps[1] * padded[1:-1] + taps[2] * padded[2:]
    conv_out = (outer_f * conv_sum).astype(jnp.bfloat16)
    if direct:
        stream_grad, grad_all, conv_all = give_back(
            row_partial.astype(jnp.bfloat16).reshape(2, experts, capacity, model_width),
            select.T,
            cotangent,
            conv_out,
            experts,
            tp_count,
        )
        out_grad = lax.dot_general(
            grad_all.reshape(groups * tok_rows, -1),
            conv_all.reshape(groups * tok_rows, -1),
            contract_first,
            preferred_element_type=jnp.float32,
        )
    else:
        half_sums = lax.psum_scatter(
            row_partial.astype(jnp.bfloat16), "tp", scatter_dimension=1, tiled=True
        ).astype(jnp.float32)
        block_width = half_sums.shape[1]
        half_grad = half_sums.reshape(groups, capacity, block_width).astype(jnp.bfloat16)
        returned = lax.all_to_all(half_grad, "sp", split_axis=0, concat_axis=0, tiled=True)
        returned = returned.reshape(experts, 2, capacity, block_width)
        select_three = select.reshape(experts, capacity, tok_rows)
        moe_part = jnp.einsum(
            "ecr,emcd->rd", select_three, returned, preferred_element_type=jnp.float32
        ).astype(jnp.bfloat16)
        moe_grad = lax.all_gather(moe_part, "tp", axis=1, tiled=True)
        stream_grad = (cotangent.astype(jnp.float32) + moe_grad.astype(jnp.float32)).astype(
            jnp.bfloat16
        )
        out_grad = lax.psum_scatter(
            lax.dot_general(
                stream_grad, conv_out, contract_first, preferred_element_type=jnp.float32
            ).astype(jnp.bfloat16),
            "sp",
            scatter_dimension=0,
            tiled=True,
        ).astype(jnp.float32)
    conv_grad = jnp.dot(stream_grad, out_weight, preferred_element_type=jnp.float32)
    outer_grad = (conv_grad * conv_sum).astype(jnp.bfloat16)
    scaled = conv_grad * outer_f
    later = from_behind(scaled[:2], "sp", -1)
    extended = jnp.concatenate([scaled, later], axis=0)
    mixed_grad = taps[2] * extended[:-2] + taps[1] * extended[1:-1] + taps[0] * extended[2:]
    inner_grad = (mixed_grad * input_f).astype(jnp.bfloat16)
    input_grad = (mixed_grad * inner_f).astype(jnp.bfloat16)
    return (gate_grad, up_grad, down_grad, out_grad, outer_grad, inner_grad, input_grad)


def solution(mesh):
    placed = (
        P("sp", None),
        P("sp", None),
        P("sp", None),
        P("sp", None),
        P("sp", None, "tp"),
        P("sp", None, "tp"),
        P("sp", "tp", None),
        P("sp", "tp"),
        P("sp", "tp"),
        P("sp", "tp"),
        P(None, "tp"),
        P(None, "tp"),
    )
    return jax.shard_map(
        per_device,
        mesh=mesh,
        in_specs=placed,
        out_specs=(
            P("sp", None, "tp"),
            P("sp", None, "tp"),
            P("sp", "tp", None),
            P("sp", "tp"),
            P("sp", "tp"),
            P("sp", "tp"),
            P("sp", "tp"),
        ),
        check_vma=False,
    )
```

```python
import functools

import jax
import jax.numpy as jnp
from jax import lax
from jax.experimental import pallas as pl
from jax.experimental.pallas import tpu as pltpu
from jax.sharding import PartitionSpec as P


def from_behind(block, axis, distance):
    devices = range(lax.axis_size(axis))
    route = [(i - distance, i) for i in devices if i - distance in devices]
    return lax.ppermute(block, axis, route)


def near_first(count):
    return sorted(range(count), key=lambda d: (min(d, count - d), d))


class Seat:
    def __init__(self, experts, pairs):
        self.sp = lax.axis_index("sp")
        self.tp = lax.axis_index("tp")
        self.half = lax.rem(self.sp, 2)
        self.expert = self.sp // 2
        self.core = lax.rem(self.tp, 2)
        self.row = self.tp // 2
        self.experts = experts
        self.pairs = pairs

    def ahead(self, distance):
        return lax.rem(self.expert + distance, self.experts)

    def behind(self, distance):
        return lax.rem(self.expert + self.experts - distance, self.experts)

    def other_expert(self, expert):
        return (expert * 2 + self.half, self.tp)

    def next_tokens(self, distance):
        groups = 2 * self.experts
        return (lax.rem(self.sp + groups + distance, groups), self.tp)

    def other_half(self):
        return (self.expert * 2 + 1 - self.half, self.tp)

    def row_ahead(self, distance):
        return lax.rem(self.row + distance, self.pairs)

    def row_behind(self, distance):
        return lax.rem(self.row + self.pairs - distance, self.pairs)

    def other_row(self, row):
        return (self.sp, row * 2 + self.core)

    def other_core(self):
        return (self.sp, self.row * 2 + 1 - self.core)


def remote(src, dst, sent, landed, device):
    return pltpu.make_async_remote_copy(
        src_ref=src,
        dst_ref=dst,
        send_sem=sent,
        recv_sem=landed,
        device_id=device,
        device_id_type=pl.DeviceIdType.MESH,
    )


def greet(peers):
    barrier = pltpu.get_barrier_semaphore()
    for peer in peers:
        pl.semaphore_signal(barrier, inc=1, device_id=peer, device_id_type=pl.DeviceIdType.MESH)
    return lambda: pl.semaphore_wait(barrier, len(peers))


def dispatch_kernel(experts, pairs, routes_ref, weights_ref, stream_ref, given_ref, mixed_ref,
                    rows_ref, cot_ref, select_ref, early_ref, send_ref, tail_ref,
                    zs, zr, xs, xr, ys, yr, ds, dr, cs, cr, own, hs, hr):
    seat = Seat(experts, pairs)
    capacity, width = send_ref.shape[2:]
    tokens = routes_ref.shape[1]
    offs = near_first(experts)
    outs = (rows_ref, cot_ref)
    all_here = greet(
        [seat.next_tokens(1), seat.next_tokens(-1)] +
        [seat.other_expert(seat.ahead(d)) for d in range(1, experts)]
        + [seat.other_half(), seat.other_core()]
        + [seat.other_row(seat.row_ahead(d)) for d in range(1, pairs)]
    )
    started = []
    tail_ref[...] = mixed_ref[tokens - tail_ref.shape[0]:, :]
    number = lax.broadcasted_iota(jnp.int32, (experts, tokens), 0)
    named = [routes_ref[k:k + 1, :] == number for k in range(2)]
    member = jnp.where(named[0] | named[1], 1.0, 0.0)
    share = jnp.where(named[0], weights_ref[0:1, :], 0.0) + jnp.where(
        named[1], weights_ref[1:2, :], 0.0
    )
    sooner = lax.broadcasted_iota(jnp.int32, (tokens, tokens), 0) < lax.broadcasted_iota(
        jnp.int32, (tokens, tokens), 1
    )
    rank = jnp.dot(
        member.astype(jnp.bfloat16),
        jnp.where(sooner, 1.0, 0.0).astype(jnp.bfloat16),
        preferred_element_type=jnp.float32,
    )
    slot = lax.broadcasted_iota(jnp.int32, (capacity, tokens), 0).astype(jnp.float32)
    mine = pl.ds(pl.multiple_of(seat.tp * width, width), width)
    slot_weight = []
    for e in range(experts):
        chosen = jnp.where(slot == rank[e:e + 1], member[e:e + 1], 0.0)
        slot_weight.append(jnp.sum(chosen * share[e:e + 1], axis=1, keepdims=True))
        select_ref[e * capacity:(e + 1) * capacity, :] = chosen.astype(jnp.bfloat16)

    def fill(kind):
        block = stream_ref[:, mine] if kind == 0 else given_ref[:, mine]
        for e in range(experts):
            picked = jnp.dot(
                select_ref[e * capacity:(e + 1) * capacity, :], block,
                preferred_element_type=jnp.float32,
            )
            if kind:
                picked = picked * slot_weight[e]
            send_ref[kind, e] = picked.astype(jnp.bfloat16)

    def place(kind, half, expert, tp):
        cols = pl.ds(pl.multiple_of(tp * width, width), width)
        return outs[kind].at[half, expert, :, cols]

    def push(src, dst, sent, landed, device):
        copy = remote(src, dst, sent, landed, device)
        copy.start()
        started.append(copy)

    def landed(spot, sem_s, sem_r):
        remote(spot, spot, sem_s, sem_r, seat.other_core()).wait_recv()

    items = [(kind, k) for kind in range(2) for k in range(experts)]
    local = []
    for kind in range(2):
        fill(kind)
        if kind == 0:
            all_here()
        spot = place(kind, seat.half, seat.expert, seat.tp)
        copy = pltpu.make_async_copy(send_ref.at[kind, seat.expert], spot, own.at[kind])
        copy.start()
        local.append(copy)
        for k in range(1, experts):
            target = seat.behind(offs[k])
            push(send_ref.at[kind, target], spot, zs.at[kind, k], zr.at[kind, k],
                 seat.other_expert(target))

    push(tail_ref, early_ref, hs.at[0], hr.at[0], seat.next_tokens(1))

    def first(kind, k):
        spot = place(kind, seat.half, seat.ahead(offs[k]), seat.tp)
        if k == 0:
            src = send_ref.at[kind, seat.expert]
        else:
            landed(spot, zs.at[kind, k], zr.at[kind, k])
            src = spot
        push(src, spot, xs.at[kind, k], xr.at[kind, k], seat.other_half())
        for d in range(1, pairs):
            push(src, spot, ys.at[kind, k, d], yr.at[kind, k, d],
                 seat.other_row(seat.row_behind(d)))
        push(src, spot, cs.at[kind, k, 0], cr.at[kind, k, 0], seat.other_core())

    def second(kind, k):
        expert = seat.ahead(offs[k])
        spot = place(kind, 1 - seat.half, expert, seat.tp)
        landed(spot, xs.at[kind, k], xr.at[kind, k])
        if k % 2 == 0:
            for d in range(1, pairs):
                push(spot, spot, ds.at[kind, k, d], dr.at[kind, k, d],
                     seat.other_row(seat.row_behind(d)))
        push(spot, spot, cs.at[kind, k, 1], cr.at[kind, k, 1], seat.other_core())
        for d in range(1, pairs):
            spot = place(kind, seat.half, expert, seat.row_ahead(d) * 2 + seat.core)
            landed(spot, ys.at[kind, k, d], yr.at[kind, k, d])
            if k % 2 == 1:
                push(spot, spot, ds.at[kind, k, d], dr.at[kind, k, d], seat.other_half())
            push(spot, spot, cs.at[kind, k, 2 * d], cr.at[kind, k, 2 * d], seat.other_core())

    def third(kind, k):
        for d in range(1, pairs):
            spot = place(kind, 1 - seat.half, seat.ahead(offs[k]),
                         seat.row_ahead(d) * 2 + seat.core)
            landed(spot, ds.at[kind, k, d], dr.at[kind, k, d])
            push(spot, spot, cs.at[kind, k, 2 * d + 1], cr.at[kind, k, 2 * d + 1],
                 seat.other_core())

    for n in range(len(items) + 2):
        if n < len(items):
            first(*items[n])
        if 1 <= n <= len(items):
            second(*items[n - 1])
        if n >= 2:
            third(*items[n - 2])
    for kind, k in items:
        expert = seat.ahead(offs[k])
        for d in range(pairs):
            tp = seat.row_ahead(d) * 2 + 1 - seat.core
            for swap in range(2):
                half = seat.half if swap == 0 else 1 - seat.half
                landed(place(kind, half, expert, tp),
                       cs.at[kind, k, 2 * d + swap], cr.at[kind, k, 2 * d + swap])
    landed(early_ref, hs.at[0], hr.at[0])
    for copy in started:
        copy.wait_send()
    for copy in local:
        copy.wait()


def return_kernel(experts, pairs, part_ref, sel_ref, cot_ref, conv_ref, sum_ref, outer_ref,
                  inner_ref, input_ref, taps_ref, weight_ref,
                  out_grad_ref, outer_grad_ref, inner_grad_ref, input_grad_ref,
                  sg_ref, g_ref, c_ref, ext_ref, late_ref, a_ref, acc_ref, b1_ref, acc2_ref, b2_ref, fin_ref, ret_ref,
                  as_, ar, b1s, b1r, b2s, b2r, zs, zr, ms, mr, gs, gr, vs, vr, us, ur, hs, hr, own):
    seat = Seat(experts, pairs)
    capacity = part_ref.shape[2]
    width = part_ref.shape[3] // (2 * pairs)
    slice_width = g_ref.shape[3]
    offs = near_first(experts)
    order = list(reversed(range(experts)))
    sp_peers = [
        (expert * 2 + half, seat.tp)
        for d in range(experts)
        for expert in [seat.ahead(d)]
        for half in ([seat.half, 1 - seat.half] if d else [1 - seat.half])
    ]
    greet(
        sp_peers + [seat.other_core()]
        + [seat.other_row(seat.row_ahead(d)) for d in range(1, pairs)]
    )()
    started = []

    def cols(tp):
        return pl.ds(pl.multiple_of(tp * width, width), width)

    def push(src, dst, sent, landed, device):
        copy = remote(src, dst, sent, landed, device)
        copy.start()
        started.append(copy)

    def landed(spot, sem_s, sem_r):
        remote(spot, spot, sem_s, sem_r, seat.other_core()).wait_recv()

    def total(*terms):
        value = terms[0].astype(jnp.float32)
        for term in terms[1:]:
            value = value + term.astype(jnp.float32)
        return value.astype(jnp.bfloat16)

    def zone(k):
        return seat.behind(offs[k])

    for k in order:
        for half in range(2):
            for row in range(pairs):
                push(part_ref.at[half, zone(k), :, cols(row * 2 + 1 - seat.core)],
                     a_ref.at[half, row, k], as_.at[half, row, k], ar.at[half, row, k],
                     seat.other_core())
    copy_conv = pltpu.make_async_copy(conv_ref, c_ref.at[seat.half, seat.expert], own.at[0])
    copy_conv.start()
    for k in range(1, experts):
        push(conv_ref, c_ref.at[seat.half, seat.expert], vs.at[k], vr.at[k],
             seat.other_expert(seat.behind(offs[k])))

    def first(k):
        for half in range(2):
            for row in range(pairs):
                landed(a_ref.at[half, row, k], as_.at[half, row, k], ar.at[half, row, k])
                acc_ref[half, row, k] = total(
                    part_ref[half, zone(k), :, cols(row * 2 + seat.core)], a_ref[half, row, k]
                )
        if k % 2 == 0:
            for row in range(pairs):
                push(acc_ref.at[1 - seat.half, row, k], b1_ref.at[k, row],
                     b1s.at[k, row], b1r.at[k, row], seat.other_half())
        else:
            for d in range(1, pairs):
                target = seat.row_behind(d)
                for half in range(2):
                    slot = 2 * (d - 1) + half
                    push(acc_ref.at[half, target, k], b1_ref.at[k, slot],
                         b1s.at[k, slot], b1r.at[k, slot], seat.other_row(target))

    def second(k):
        if k % 2 == 0:
            for row in range(pairs):
                landed(b1_ref.at[k, row], b1s.at[k, row], b1r.at[k, row])
                acc2_ref[k, row] = total(acc_ref[seat.half, row, k], b1_ref[k, row])
            for d in range(1, pairs):
                target = seat.row_behind(d)
                push(acc2_ref.at[k, target], b2_ref.at[k, d - 1], b2s.at[k, d - 1],
                     b2r.at[k, d - 1], seat.other_row(target))
        else:
            for half in range(2):
                terms = [acc_ref[half, seat.row, k]]
                for d in range(1, pairs):
                    slot = 2 * (d - 1) + half
                    landed(b1_ref.at[k, slot], b1s.at[k, slot], b1r.at[k, slot])
                    terms.append(b1_ref[k, slot])
                acc2_ref[k, half] = total(*terms)
            push(acc2_ref.at[k, 1 - seat.half], b2_ref.at[k, 0], b2s.at[k, 0], b2r.at[k, 0],
                 seat.other_half())

    def third(k):
        count = pairs - 1 if k % 2 == 0 else 1
        terms = [acc2_ref[k, seat.row if k % 2 == 0 else seat.half]]
        for slot in range(count):
            landed(b2_ref.at[k, slot], b2s.at[k, slot], b2r.at[k, slot])
            terms.append(b2_ref[k, slot])
        rows = pl.ds(pl.multiple_of(seat.expert * capacity, 16), capacity)
        if k == 0:
            ret_ref[rows, :] = total(*terms)
        else:
            fin_ref[k] = total(*terms)
            push(fin_ref.at[k], ret_ref.at[rows, :], zs.at[k], zr.at[k],
                 seat.other_expert(zone(k)))

    for n in range(experts + 2):
        if n < experts:
            first(order[n])
        if 1 <= n <= experts:
            second(order[n - 1])
        if n >= 2:
            third(order[n - 2])
    copy_conv.wait()
    for k in range(experts):
        expert = seat.ahead(offs[k])
        spot = c_ref.at[seat.half, expert]
        if k:
            landed(spot, vs.at[k], vr.at[k])
        push(spot, spot, us.at[k], ur.at[k], seat.other_half())
    for k in range(1, experts):
        rows = pl.ds(pl.multiple_of(seat.ahead(offs[k]) * capacity, 16), capacity)
        landed(ret_ref.at[rows, :], zs.at[k], zr.at[k])
    over_first = (((0,), (0,)), ((), ()))
    moe = lax.dot_general(
        sel_ref[...], ret_ref[...], over_first, preferred_element_type=jnp.float32
    )
    mine = cols(seat.tp)
    sg_ref[:, mine] = total(cot_ref[:, mine], moe.astype(jnp.bfloat16))
    for d in range(1, pairs):
        push(sg_ref.at[:, mine], sg_ref.at[:, mine], ms.at[2 * d], mr.at[2 * d],
             seat.other_row(seat.row_behind(d)))
    push(sg_ref.at[:, mine], sg_ref.at[:, mine], ms.at[0], mr.at[0], seat.other_core())
    for d in range(1, pairs):
        theirs = sg_ref.at[:, cols(seat.row_ahead(d) * 2 + seat.core)]
        landed(theirs, ms.at[2 * d], mr.at[2 * d])
        push(theirs, theirs, ms.at[2 * d + 1], mr.at[2 * d + 1], seat.other_core())
    for d in range(pairs):
        slot = 0 if d == 0 else 2 * d + 1
        theirs = sg_ref.at[:, cols(seat.row_ahead(d) * 2 + 1 - seat.core)]
        landed(theirs, ms.at[slot], mr.at[slot])

    def piece(sp):
        return sg_ref.at[:, pl.ds(pl.multiple_of(sp * slice_width, 128), slice_width)]

    for k in range(experts):
        expert = seat.behind(offs[k])
        for swap in range(2):
            if k == 0 and swap == 0:
                continue
            half = seat.half if swap == 0 else 1 - seat.half
            push(piece(expert * 2 + half), g_ref.at[seat.half, seat.expert],
                 gs.at[k, swap], gr.at[k, swap], (expert * 2 + half, seat.tp))
    keep = pltpu.make_async_copy(piece(seat.sp), g_ref.at[seat.half, seat.expert], own.at[1])
    keep.start()
    tokens = sum_ref.shape[0]
    border = late_ref.shape[0]
    conv_grad = jnp.dot(sg_ref[...], weight_ref[...], preferred_element_type=jnp.float32)
    ext_ref[0:tokens, :] = conv_grad * outer_ref[...].astype(jnp.float32)
    push(ext_ref.at[0:border, :], late_ref, hs.at[0], hr.at[0], seat.next_tokens(-1))
    outer_grad_ref[...] = (conv_grad * sum_ref[...]).astype(jnp.bfloat16)
    keep.wait()
    out_grad_ref[...] = jnp.zeros_like(out_grad_ref)

    def add_out(half, expert):
        out_grad_ref[...] += lax.dot_general(
            g_ref[half, expert], c_ref[half, expert], over_first,
            preferred_element_type=jnp.float32,
        )

    add_out(seat.half, seat.expert)
    landed(late_ref, hs.at[0], hr.at[0])
    ext_ref[tokens:tokens + border, :] = jnp.where(
        seat.sp == 2 * experts - 1, 0.0, late_ref[...]
    )
    mixed_grad = taps_ref[2:3, :] * ext_ref[0:tokens, :]
    mixed_grad = mixed_grad + taps_ref[1:2, :] * ext_ref[1:tokens + 1, :]
    mixed_grad = mixed_grad + taps_ref[0:1, :] * ext_ref[2:tokens + 2, :]
    inner_grad_ref[...] = (mixed_grad * input_ref[...].astype(jnp.float32)).astype(jnp.bfloat16)
    input_grad_ref[...] = (mixed_grad * inner_ref[...].astype(jnp.float32)).astype(jnp.bfloat16)
    for k in range(experts):
        expert = seat.ahead(offs[k])
        landed(c_ref.at[1 - seat.half, expert], us.at[k], ur.at[k])
        for swap in range(2):
            if k == 0 and swap == 0:
                continue
            half = seat.half if swap == 0 else 1 - seat.half
            landed(g_ref.at[half, expert], gs.at[k, swap], gr.at[k, swap])
            add_out(half, expert)
    for copy in started:
        copy.wait_send()


def vmem(count):
    return [pl.BlockSpec(memory_space=pltpu.VMEM)] * count


def sems(*shape):
    return pltpu.SemaphoreType.DMA(shape)


def dispatch(routes, route_weights, stream, cotangent, mixed, capacity, experts, tp_count):
    pairs = tp_count // 2
    tokens, model_width = stream.shape
    width = model_width // tp_count
    border = min(8, tokens)
    shape = jax.ShapeDtypeStruct((2, experts, capacity, model_width), jnp.bfloat16)
    halo = (border, mixed.shape[1])
    flat, rowed = (2, experts), (2, experts, pairs)
    cored = (2, experts, 2 * pairs)
    return pl.pallas_call(
        functools.partial(dispatch_kernel, experts, pairs),
        out_shape=(
            shape,
            shape,
            jax.ShapeDtypeStruct((experts * capacity, tokens), jnp.bfloat16),
            jax.ShapeDtypeStruct(halo, jnp.float32),
        ),
        in_specs=vmem(5),
        out_specs=tuple(vmem(4)),
        scratch_shapes=[
            pltpu.VMEM((2, experts, capacity, width), jnp.bfloat16),
            pltpu.VMEM(halo, jnp.float32),
        ]
        + [
            sems(*s)
            for s in (
                flat, flat, flat, flat, rowed, rowed, rowed, rowed, cored, cored,
                (2,), (1,), (1,),
            )
        ],
        compiler_params=pltpu.CompilerParams(
            collective_id=0, has_side_effects=True, vmem_limit_bytes=32 * 1024 * 1024
        ),
    )(routes.T, route_weights.T, stream, cotangent, mixed)


def give_back(part, select, cotangent, conv_out, conv_sum, outer, inner, given, taps,
              out_weight, experts, tp_count):
    pairs = tp_count // 2
    _, _, capacity, model_width = part.shape
    tokens, channels = conv_out.shape
    width = model_width // tp_count
    slice_width = model_width // (2 * experts)
    border = min(8, tokens)
    most = max(pairs, 2 * (pairs - 1))
    late = max(pairs - 1, 1)
    bf16 = jnp.bfloat16
    own_channels = jax.ShapeDtypeStruct((tokens, channels), bf16)
    return pl.pallas_call(
        functools.partial(return_kernel, experts, pairs),
        out_shape=(
            jax.ShapeDtypeStruct((slice_width, channels), jnp.float32),
            own_channels,
            own_channels,
            own_channels,
        ),
        in_specs=vmem(10),
        out_specs=tuple(vmem(4)),
        scratch_shapes=[
            pltpu.VMEM((tokens, model_width), bf16),
            pltpu.VMEM((2, experts, tokens, slice_width), bf16),
            pltpu.VMEM((2, experts, tokens, channels), bf16),
            pltpu.VMEM((tokens + border, channels), jnp.float32),
            pltpu.VMEM((border, channels), jnp.float32),
            pltpu.VMEM((2, pairs, experts, capacity, width), bf16),
            pltpu.VMEM((2, pairs, experts, capacity, width), bf16),
            pltpu.VMEM((experts, most, capacity, width), bf16),
            pltpu.VMEM((experts, max(pairs, 2), capacity, width), bf16),
            pltpu.VMEM((experts, late, capacity, width), bf16),
            pltpu.VMEM((experts, capacity, width), bf16),
            pltpu.VMEM((experts * capacity, width), bf16),
        ]
        + [
            sems(*s)
            for shape in (
                (2, pairs, experts), (experts, most), (experts, late), (experts,),
                (2 * pairs,), (experts, 2), (experts,), (experts,), (1,),
            )
            for s in (shape, shape)
        ]
        + [sems(2)],
        compiler_params=pltpu.CompilerParams(
            collective_id=1, has_side_effects=True, vmem_limit_bytes=40 * 1024 * 1024
        ),
    )(part, select, cotangent, conv_out, conv_sum, outer, inner, given, taps, out_weight)


def per_device(
    cotangent,
    stream,
    routes,
    route_weights,
    gate_weight,
    up_weight,
    down_weight,
    outer_gate,
    inner_gate,
    conv_input,
    conv_taps,
    out_weight,
):
    groups = lax.axis_size("sp")
    tp_count = lax.axis_size("tp")
    experts = groups // 2
    tok_rows = stream.shape[0]
    model_width = stream.shape[1]
    capacity = 3 * tok_rows // experts
    slot_total = experts * capacity
    contract_first = (((0,), (0,)), ((), ()))
    contract_last = (((1,), (1,)), ((), ()))
    block_width = model_width // tp_count
    slots = groups * capacity
    direct = tp_count % 2 == 0 and capacity % 16 == 0 and block_width % 128 == 0
    taps = conv_taps.astype(jnp.float32)
    outer_f = outer_gate.astype(jnp.float32)
    inner_f = inner_gate.astype(jnp.float32)
    input_f = conv_input.astype(jnp.float32)
    mixed = inner_f * input_f
    if direct:
        routed_rows, routed_cot, select, early = dispatch(
            routes, route_weights, stream, cotangent, mixed, capacity, experts, tp_count
        )
        routed_rows = routed_rows.reshape(slots, model_width)
        routed_cot = routed_cot.reshape(slots, model_width)
        earlier = jnp.where(lax.axis_index("sp") == 0, 0.0, early[-2:])
    else:
        flat_routes = routes.reshape(-1)
        choose = (flat_routes[:, None] == jnp.arange(experts, dtype=jnp.int32)[None, :]).astype(
            jnp.int32
        )
        before = jnp.cumsum(choose, axis=0) - choose
        slot_place = flat_routes * capacity + jnp.sum(before * choose, axis=1)
        slot_table = (jnp.arange(slot_total, dtype=jnp.int32)[:, None] == slot_place[None, :]).astype(
            jnp.float32
        )
        select = jnp.sum(slot_table.reshape(slot_total, tok_rows, 2), axis=2).astype(jnp.bfloat16)
        slot_weight = jnp.sum(slot_table * route_weights.reshape(-1)[None, :], axis=1)
        offset = lax.axis_index("tp") * block_width
        rows_part = lax.dynamic_slice_in_dim(stream, offset, block_width, 1)
        cot_part = lax.dynamic_slice_in_dim(cotangent, offset, block_width, 1)
        sent_rows = jnp.dot(select, rows_part, preferred_element_type=jnp.float32).astype(jnp.bfloat16)
        sent_cot = (
            jnp.dot(select, cot_part, preferred_element_type=jnp.float32) * slot_weight[:, None]
        ).astype(jnp.bfloat16)
        sent_rows = jnp.repeat(sent_rows.reshape(experts, capacity, -1), 2, axis=0)
        sent_cot = jnp.repeat(sent_cot.reshape(experts, capacity, -1), 2, axis=0)
        recv_rows, recv_cot = (
            lax.all_to_all(sent_rows, "sp", split_axis=0, concat_axis=0, tiled=True),
            lax.all_to_all(sent_cot, "sp", split_axis=0, concat_axis=0, tiled=True),
        )
        recv_rows, recv_cot = (
            lax.all_gather(recv_rows, "tp", axis=2, tiled=True),
            lax.all_gather(recv_cot, "tp", axis=2, tiled=True),
        )
        routed_rows = recv_rows.reshape(slots, model_width)
        routed_cot = recv_cot.reshape(slots, model_width)
        earlier = from_behind(mixed[-2:], "sp", 1)
    gate_local = gate_weight[0]
    up_local = up_weight[0]
    down_local = down_weight[0]
    gate_pre = jnp.dot(routed_rows, gate_local, preferred_element_type=jnp.float32)
    up_pre = jnp.dot(routed_rows, up_local, preferred_element_type=jnp.float32)
    hidden_grad = lax.dot_general(
        routed_cot, down_local, contract_last, preferred_element_type=jnp.float32
    )
    sigma = jax.nn.sigmoid(gate_pre)
    silu_gate = gate_pre * sigma
    hidden = (silu_gate * up_pre).astype(jnp.bfloat16)
    up_delta = (hidden_grad * silu_gate).astype(jnp.bfloat16)
    gate_delta = (hidden_grad * up_pre * sigma * (1.0 + gate_pre * (1.0 - sigma))).astype(
        jnp.bfloat16
    )
    gate_grad = lax.dot_general(
        routed_rows, gate_delta, contract_first, preferred_element_type=jnp.float32
    ).astype(jnp.bfloat16)[None]
    up_grad = lax.dot_general(
        routed_rows, up_delta, contract_first, preferred_element_type=jnp.float32
    ).astype(jnp.bfloat16)[None]
    down_grad = lax.dot_general(
        hidden, routed_cot, contract_first, preferred_element_type=jnp.float32
    ).astype(jnp.bfloat16)[None]
    row_partial = lax.dot_general(
        gate_delta, gate_local, contract_last, preferred_element_type=jnp.float32
    )
    row_partial = row_partial + lax.dot_general(
        up_delta, up_local, contract_last, preferred_element_type=jnp.float32
    )
    padded = jnp.concatenate([earlier, mixed], axis=0)
    conv_sum = taps[0] * padded[:-2] + taps[1] * padded[1:-1] + taps[2] * padded[2:]
    conv_out = (outer_f * conv_sum).astype(jnp.bfloat16)
    if direct:
        out_grad, outer_grad, inner_grad, input_grad = give_back(
            row_partial.astype(jnp.bfloat16).reshape(2, experts, capacity, model_width),
            select,
            cotangent,
            conv_out,
            conv_sum,
            outer_gate,
            inner_gate,
            conv_input,
            taps,
            out_weight,
            experts,
            tp_count,
        )
    else:
        half_sums = lax.psum_scatter(
            row_partial.astype(jnp.bfloat16), "tp", scatter_dimension=1, tiled=True
        ).astype(jnp.float32)
        block_width = half_sums.shape[1]
        half_grad = half_sums.reshape(groups, capacity, block_width).astype(jnp.bfloat16)
        returned = lax.all_to_all(half_grad, "sp", split_axis=0, concat_axis=0, tiled=True)
        returned = returned.reshape(experts, 2, capacity, block_width)
        select_three = select.reshape(experts, capacity, tok_rows)
        moe_part = jnp.einsum(
            "ecr,emcd->rd", select_three, returned, preferred_element_type=jnp.float32
        ).astype(jnp.bfloat16)
        moe_grad = lax.all_gather(moe_part, "tp", axis=1, tiled=True)
        stream_grad = (cotangent.astype(jnp.float32) + moe_grad.astype(jnp.float32)).astype(
            jnp.bfloat16
        )
        out_grad = lax.psum_scatter(
            lax.dot_general(
                stream_grad, conv_out, contract_first, preferred_element_type=jnp.float32
            ).astype(jnp.bfloat16),
            "sp",
            scatter_dimension=0,
            tiled=True,
        ).astype(jnp.float32)
        conv_grad = jnp.dot(stream_grad, out_weight, preferred_element_type=jnp.float32)
        outer_grad = (conv_grad * conv_sum).astype(jnp.bfloat16)
        scaled = conv_grad * outer_f
        later = from_behind(scaled[:2], "sp", -1)
        extended = jnp.concatenate([scaled, later], axis=0)
        mixed_grad = taps[2] * extended[:-2] + taps[1] * extended[1:-1] + taps[0] * extended[2:]
        inner_grad = (mixed_grad * input_f).astype(jnp.bfloat16)
        input_grad = (mixed_grad * inner_f).astype(jnp.bfloat16)
    return (gate_grad, up_grad, down_grad, out_grad, outer_grad, inner_grad, input_grad)


def solution(mesh):
    placed = (
        P("sp", None),
        P("sp", None),
        P("sp", None),
        P("sp", None),
        P("sp", None, "tp"),
        P("sp", None, "tp"),
        P("sp", "tp", None),
        P("sp", "tp"),
        P("sp", "tp"),
        P("sp", "tp"),
        P(None, "tp"),
        P(None, "tp"),
    )
    return jax.shard_map(
        per_device,
        mesh=mesh,
        in_specs=placed,
        out_specs=(
            P("sp", None, "tp"),
            P("sp", None, "tp"),
            P("sp", "tp", None),
            P("sp", "tp"),
            P("sp", "tp"),
            P("sp", "tp"),
            P("sp", "tp"),
        ),
        check_vma=False,
    )
```

```python
import functools

import jax
import jax.numpy as jnp
from jax import lax
from jax.experimental import pallas as pl
from jax.experimental.pallas import tpu as pltpu
from jax.sharding import PartitionSpec as P


def from_behind(block, axis, distance):
    devices = range(lax.axis_size(axis))
    route = [(i - distance, i) for i in devices if i - distance in devices]
    return lax.ppermute(block, axis, route)


def near_first(count):
    return sorted(range(count), key=lambda d: (min(d, count - d), d))


class Seat:
    def __init__(self, experts, pairs):
        self.sp = lax.axis_index("sp")
        self.tp = lax.axis_index("tp")
        self.half = lax.rem(self.sp, 2)
        self.expert = self.sp // 2
        self.core = lax.rem(self.tp, 2)
        self.row = self.tp // 2
        self.experts = experts
        self.pairs = pairs

    def ahead(self, distance):
        return lax.rem(self.expert + distance, self.experts)

    def behind(self, distance):
        return lax.rem(self.expert + self.experts - distance, self.experts)

    def other_expert(self, expert):
        return (expert * 2 + self.half, self.tp)

    def next_tokens(self, distance):
        groups = 2 * self.experts
        return (lax.rem(self.sp + groups + distance, groups), self.tp)

    def other_half(self):
        return (self.expert * 2 + 1 - self.half, self.tp)

    def row_ahead(self, distance):
        return lax.rem(self.row + distance, self.pairs)

    def row_behind(self, distance):
        return lax.rem(self.row + self.pairs - distance, self.pairs)

    def other_row(self, row):
        return (self.sp, row * 2 + self.core)

    def other_core(self):
        return (self.sp, self.row * 2 + 1 - self.core)


def remote(src, dst, sent, landed, device):
    return pltpu.make_async_remote_copy(
        src_ref=src,
        dst_ref=dst,
        send_sem=sent,
        recv_sem=landed,
        device_id=device,
        device_id_type=pl.DeviceIdType.MESH,
    )


def greet(peers):
    barrier = pltpu.get_barrier_semaphore()
    for peer in peers:
        pl.semaphore_signal(barrier, inc=1, device_id=peer, device_id_type=pl.DeviceIdType.MESH)
    return lambda: pl.semaphore_wait(barrier, len(peers))


def dispatch_kernel(experts, pairs, routes_hbm, weights_hbm, stream_hbm, given_hbm, inner_hbm, input_hbm,
                    rows_ref, cot_ref, select_ref, early_ref, send_ref, tail_ref,
                    routes_ref, weights_ref, block_ref, edge_ref,
                    zs, zr, xs, xr, ys, yr, ds, dr, cs, cr, own, hs, hr, ls):
    seat = Seat(experts, pairs)
    capacity, width = send_ref.shape[2:]
    tokens = routes_ref.shape[1]
    offs = near_first(experts)
    outs = (rows_ref, cot_ref)
    all_here = greet(
        [seat.next_tokens(1), seat.next_tokens(-1)] +
        [seat.other_expert(seat.ahead(d)) for d in range(1, experts)]
        + [seat.other_half(), seat.other_core()]
        + [seat.other_row(seat.row_ahead(d)) for d in range(1, pairs)]
    )
    started = []
    mine = pl.ds(pl.multiple_of(seat.tp * width, width), width)
    edge = pl.ds(tokens - tail_ref.shape[0], tail_ref.shape[0])
    loads = [
        pltpu.make_async_copy(src, dst, ls.at[n])
        for n, (src, dst) in enumerate((
            (routes_hbm, routes_ref),
            (weights_hbm, weights_ref),
            (stream_hbm.at[:, mine], block_ref.at[0]),
            (inner_hbm.at[edge, :], edge_ref.at[0]),
            (input_hbm.at[edge, :], edge_ref.at[1]),
            (given_hbm.at[:, mine], block_ref.at[1]),
        ))
    ]
    for load in loads:
        load.start()
    for load in loads:
        load.wait()
    tail_ref[...] = edge_ref[0].astype(jnp.float32) * edge_ref[1].astype(jnp.float32)
    number = lax.broadcasted_iota(jnp.int32, (experts, tokens), 0)
    named = [routes_ref[k:k + 1, :] == number for k in range(2)]
    member = jnp.where(named[0] | named[1], 1.0, 0.0)
    share = jnp.where(named[0], weights_ref[0:1, :], 0.0) + jnp.where(
        named[1], weights_ref[1:2, :], 0.0
    )
    sooner = lax.broadcasted_iota(jnp.int32, (tokens, tokens), 0) < lax.broadcasted_iota(
        jnp.int32, (tokens, tokens), 1
    )
    rank = jnp.dot(
        member.astype(jnp.bfloat16),
        jnp.where(sooner, 1.0, 0.0).astype(jnp.bfloat16),
        preferred_element_type=jnp.float32,
    )
    slot = lax.broadcasted_iota(jnp.int32, (capacity, tokens), 0).astype(jnp.float32)
    slot_weight = []
    for e in range(experts):
        chosen = jnp.where(slot == rank[e:e + 1], member[e:e + 1], 0.0)
        slot_weight.append(jnp.sum(chosen * share[e:e + 1], axis=1, keepdims=True))
        select_ref[e * capacity:(e + 1) * capacity, :] = chosen.astype(jnp.bfloat16)

    def fill(kind):
        block = block_ref[kind]
        for e in range(experts):
            picked = jnp.dot(
                select_ref[e * capacity:(e + 1) * capacity, :], block,
                preferred_element_type=jnp.float32,
            )
            if kind:
                picked = picked * slot_weight[e]
            send_ref[kind, e] = picked.astype(jnp.bfloat16)

    def place(kind, half, expert, tp):
        cols = pl.ds(pl.multiple_of(tp * width, width), width)
        return outs[kind].at[half, expert, :, cols]

    def push(src, dst, sent, landed, device):
        copy = remote(src, dst, sent, landed, device)
        copy.start()
        started.append(copy)

    def landed(spot, sem_s, sem_r):
        remote(spot, spot, sem_s, sem_r, seat.other_core()).wait_recv()

    items = [(kind, k) for kind in range(2) for k in range(experts)]
    local = []
    for kind in range(2):
        fill(kind)
        if kind == 0:
            all_here()
        spot = place(kind, seat.half, seat.expert, seat.tp)
        copy = pltpu.make_async_copy(send_ref.at[kind, seat.expert], spot, own.at[kind])
        copy.start()
        local.append(copy)
        for k in range(1, experts):
            target = seat.behind(offs[k])
            push(send_ref.at[kind, target], spot, zs.at[kind, k], zr.at[kind, k],
                 seat.other_expert(target))

    push(tail_ref, early_ref, hs.at[0], hr.at[0], seat.next_tokens(1))

    def first(kind, k):
        spot = place(kind, seat.half, seat.ahead(offs[k]), seat.tp)
        if k == 0:
            src = send_ref.at[kind, seat.expert]
        else:
            landed(spot, zs.at[kind, k], zr.at[kind, k])
            src = spot
        push(src, spot, xs.at[kind, k], xr.at[kind, k], seat.other_half())
        for d in range(1, pairs):
            push(src, spot, ys.at[kind, k, d], yr.at[kind, k, d],
                 seat.other_row(seat.row_behind(d)))
        push(src, spot, cs.at[kind, k, 0], cr.at[kind, k, 0], seat.other_core())

    def second(kind, k):
        expert = seat.ahead(offs[k])
        spot = place(kind, 1 - seat.half, expert, seat.tp)
        landed(spot, xs.at[kind, k], xr.at[kind, k])
        if k % 2 == 0:
            for d in range(1, pairs):
                push(spot, spot, ds.at[kind, k, d], dr.at[kind, k, d],
                     seat.other_row(seat.row_behind(d)))
        push(spot, spot, cs.at[kind, k, 1], cr.at[kind, k, 1], seat.other_core())
        for d in range(1, pairs):
            spot = place(kind, seat.half, expert, seat.row_ahead(d) * 2 + seat.core)
            landed(spot, ys.at[kind, k, d], yr.at[kind, k, d])
            if k % 2 == 1:
                push(spot, spot, ds.at[kind, k, d], dr.at[kind, k, d], seat.other_half())
            push(spot, spot, cs.at[kind, k, 2 * d], cr.at[kind, k, 2 * d], seat.other_core())

    def third(kind, k):
        for d in range(1, pairs):
            spot = place(kind, 1 - seat.half, seat.ahead(offs[k]),
                         seat.row_ahead(d) * 2 + seat.core)
            landed(spot, ds.at[kind, k, d], dr.at[kind, k, d])
            push(spot, spot, cs.at[kind, k, 2 * d + 1], cr.at[kind, k, 2 * d + 1],
                 seat.other_core())

    for n in range(len(items) + 2):
        if n < len(items):
            first(*items[n])
        if 1 <= n <= len(items):
            second(*items[n - 1])
        if n >= 2:
            third(*items[n - 2])
    for kind, k in items:
        expert = seat.ahead(offs[k])
        for d in range(pairs):
            tp = seat.row_ahead(d) * 2 + 1 - seat.core
            for swap in range(2):
                half = seat.half if swap == 0 else 1 - seat.half
                landed(place(kind, half, expert, tp),
                       cs.at[kind, k, 2 * d + swap], cr.at[kind, k, 2 * d + swap])
    landed(early_ref, hs.at[0], hr.at[0])
    for copy in started:
        copy.wait_send()
    for copy in local:
        copy.wait()


def return_kernel(experts, pairs, part_ref, sel_ref, cot_hbm, conv_ref, sum_ref, outer_ref,
                  inner_ref, input_ref, taps_ref, weight_hbm,
                  rows_ref, routed_ref, hidden_ref, gate_ref, up_ref,
                  gate_grad_ref, up_grad_ref, down_grad_ref, out_grad_ref, outer_grad_ref, inner_grad_ref, input_grad_ref,
                  cot_ref, weight_ref, sg_ref, g_ref, c_ref, ext_ref, late_ref, a_ref, acc_ref, b1_ref, acc2_ref, b2_ref, fin_ref, ret_ref,
                  as_, ar, b1s, b1r, b2s, b2r, zs, zr, ms, mr, gs, gr, vs, vr, us, ur, hs, hr, own):
    seat = Seat(experts, pairs)
    capacity = part_ref.shape[2]
    width = part_ref.shape[3] // (2 * pairs)
    slice_width = g_ref.shape[3]
    offs = near_first(experts)
    order = list(reversed(range(experts)))
    sp_peers = [
        (expert * 2 + half, seat.tp)
        for d in range(experts)
        for expert in [seat.ahead(d)]
        for half in ([seat.half, 1 - seat.half] if d else [1 - seat.half])
    ]
    greet(
        sp_peers + [seat.other_core()]
        + [seat.other_row(seat.row_ahead(d)) for d in range(1, pairs)]
    )()
    started = []
    over_first = (((0,), (0,)), ((), ()))
    step = 512 if rows_ref.shape[1] % 512 == 0 else rows_ref.shape[1]
    pieces = [(n, at) for n in range(3) for at in range(0, rows_ref.shape[1], step)]

    def work(count):
        for n, at in [pieces.pop(0) for _ in range(min(count, len(pieces)))]:
            span = slice(at, at + step)
            if n < 2:
                delta, out = ((gate_ref, gate_grad_ref), (up_ref, up_grad_ref))[n]
                out[span, :] = lax.dot_general(
                    rows_ref[:, span], delta[...], over_first,
                    preferred_element_type=jnp.float32,
                ).astype(jnp.bfloat16)
            else:
                down_grad_ref[:, span] = lax.dot_general(
                    hidden_ref[...], routed_ref[:, span], over_first,
                    preferred_element_type=jnp.float32,
                ).astype(jnp.bfloat16)

    def cols(tp):
        return pl.ds(pl.multiple_of(tp * width, width), width)

    def push(src, dst, sent, landed, device):
        copy = remote(src, dst, sent, landed, device)
        copy.start()
        started.append(copy)

    def landed(spot, sem_s, sem_r):
        remote(spot, spot, sem_s, sem_r, seat.other_core()).wait_recv()

    def total(*terms):
        value = terms[0].astype(jnp.float32)
        for term in terms[1:]:
            value = value + term.astype(jnp.float32)
        return value.astype(jnp.bfloat16)

    def zone(k):
        return seat.behind(offs[k])

    for k in order:
        for half in range(2):
            for row in range(pairs):
                push(part_ref.at[half, zone(k), :, cols(row * 2 + 1 - seat.core)],
                     a_ref.at[half, row, k], as_.at[half, row, k], ar.at[half, row, k],
                     seat.other_core())
    copy_conv = pltpu.make_async_copy(conv_ref, c_ref.at[seat.half, seat.expert], own.at[0])
    copy_conv.start()
    mine = cols(seat.tp)
    load_cot = pltpu.make_async_copy(cot_hbm.at[:, mine], cot_ref, own.at[2])
    load_weight = pltpu.make_async_copy(weight_hbm, weight_ref, own.at[3])
    load_cot.start()
    load_weight.start()
    for k in range(1, experts):
        push(conv_ref, c_ref.at[seat.half, seat.expert], vs.at[k], vr.at[k],
             seat.other_expert(seat.behind(offs[k])))

    def first(k):
        for half in range(2):
            for row in range(pairs):
                landed(a_ref.at[half, row, k], as_.at[half, row, k], ar.at[half, row, k])
                acc_ref[half, row, k] = total(
                    part_ref[half, zone(k), :, cols(row * 2 + seat.core)], a_ref[half, row, k]
                )
        if k % 2 == 0:
            for row in range(pairs):
                push(acc_ref.at[1 - seat.half, row, k], b1_ref.at[k, row],
                     b1s.at[k, row], b1r.at[k, row], seat.other_half())
        else:
            for d in range(1, pairs):
                target = seat.row_behind(d)
                for half in range(2):
                    slot = 2 * (d - 1) + half
                    push(acc_ref.at[half, target, k], b1_ref.at[k, slot],
                         b1s.at[k, slot], b1r.at[k, slot], seat.other_row(target))

    def second(k):
        if k % 2 == 0:
            for row in range(pairs):
                landed(b1_ref.at[k, row], b1s.at[k, row], b1r.at[k, row])
                acc2_ref[k, row] = total(acc_ref[seat.half, row, k], b1_ref[k, row])
            for d in range(1, pairs):
                target = seat.row_behind(d)
                push(acc2_ref.at[k, target], b2_ref.at[k, d - 1], b2s.at[k, d - 1],
                     b2r.at[k, d - 1], seat.other_row(target))
        else:
            for half in range(2):
                terms = [acc_ref[half, seat.row, k]]
                for d in range(1, pairs):
                    slot = 2 * (d - 1) + half
                    landed(b1_ref.at[k, slot], b1s.at[k, slot], b1r.at[k, slot])
                    terms.append(b1_ref[k, slot])
                acc2_ref[k, half] = total(*terms)
            push(acc2_ref.at[k, 1 - seat.half], b2_ref.at[k, 0], b2s.at[k, 0], b2r.at[k, 0],
                 seat.other_half())

    def third(k):
        count = pairs - 1 if k % 2 == 0 else 1
        terms = [acc2_ref[k, seat.row if k % 2 == 0 else seat.half]]
        for slot in range(count):
            landed(b2_ref.at[k, slot], b2s.at[k, slot], b2r.at[k, slot])
            terms.append(b2_ref[k, slot])
        rows = pl.ds(pl.multiple_of(seat.expert * capacity, 16), capacity)
        if k == 0:
            ret_ref[rows, :] = total(*terms)
        else:
            fin_ref[k] = total(*terms)
            push(fin_ref.at[k], ret_ref.at[rows, :], zs.at[k], zr.at[k],
                 seat.other_expert(zone(k)))

    for n in range(experts + 2):
        if n < experts:
            first(order[n])
        work(1)
        if 1 <= n <= experts:
            second(order[n - 1])
        if n >= 2:
            third(order[n - 2])
    copy_conv.wait()
    for k in range(experts):
        expert = seat.ahead(offs[k])
        spot = c_ref.at[seat.half, expert]
        if k:
            landed(spot, vs.at[k], vr.at[k])
        push(spot, spot, us.at[k], ur.at[k], seat.other_half())
    work(2)
    load_cot.wait()
    load_weight.wait()
    for k in range(1, experts):
        rows = pl.ds(pl.multiple_of(seat.ahead(offs[k]) * capacity, 16), capacity)
        landed(ret_ref.at[rows, :], zs.at[k], zr.at[k])
    moe = lax.dot_general(
        sel_ref[...], ret_ref[...], over_first, preferred_element_type=jnp.float32
    )
    sg_ref[:, mine] = total(cot_ref[...], moe.astype(jnp.bfloat16))
    for d in range(1, pairs):
        push(sg_ref.at[:, mine], sg_ref.at[:, mine], ms.at[2 * d], mr.at[2 * d],
             seat.other_row(seat.row_behind(d)))
    push(sg_ref.at[:, mine], sg_ref.at[:, mine], ms.at[0], mr.at[0], seat.other_core())
    work(2)
    for d in range(1, pairs):
        theirs = sg_ref.at[:, cols(seat.row_ahead(d) * 2 + seat.core)]
        landed(theirs, ms.at[2 * d], mr.at[2 * d])
        push(theirs, theirs, ms.at[2 * d + 1], mr.at[2 * d + 1], seat.other_core())
    for d in range(pairs):
        slot = 0 if d == 0 else 2 * d + 1
        theirs = sg_ref.at[:, cols(seat.row_ahead(d) * 2 + 1 - seat.core)]
        landed(theirs, ms.at[slot], mr.at[slot])

    def piece(sp):
        return sg_ref.at[:, pl.ds(pl.multiple_of(sp * slice_width, 128), slice_width)]

    for k in range(experts):
        expert = seat.behind(offs[k])
        for swap in range(2):
            if k == 0 and swap == 0:
                continue
            half = seat.half if swap == 0 else 1 - seat.half
            push(piece(expert * 2 + half), g_ref.at[seat.half, seat.expert],
                 gs.at[k, swap], gr.at[k, swap], (expert * 2 + half, seat.tp))
    keep = pltpu.make_async_copy(piece(seat.sp), g_ref.at[seat.half, seat.expert], own.at[1])
    keep.start()
    tokens = sum_ref.shape[0]
    border = late_ref.shape[0]
    conv_grad = jnp.dot(sg_ref[...], weight_ref[...], preferred_element_type=jnp.float32)
    ext_ref[0:tokens, :] = conv_grad * outer_ref[...].astype(jnp.float32)
    push(ext_ref.at[0:border, :], late_ref, hs.at[0], hr.at[0], seat.next_tokens(-1))
    outer_grad_ref[...] = (conv_grad * sum_ref[...]).astype(jnp.bfloat16)
    keep.wait()
    out_grad_ref[...] = jnp.zeros_like(out_grad_ref)

    def add_out(half, expert):
        out_grad_ref[...] += lax.dot_general(
            g_ref[half, expert], c_ref[half, expert], over_first,
            preferred_element_type=jnp.float32,
        )

    add_out(seat.half, seat.expert)
    work(len(pieces))
    landed(late_ref, hs.at[0], hr.at[0])
    ext_ref[tokens:tokens + border, :] = jnp.where(
        seat.sp == 2 * experts - 1, 0.0, late_ref[...]
    )
    mixed_grad = taps_ref[2:3, :] * ext_ref[0:tokens, :]
    mixed_grad = mixed_grad + taps_ref[1:2, :] * ext_ref[1:tokens + 1, :]
    mixed_grad = mixed_grad + taps_ref[0:1, :] * ext_ref[2:tokens + 2, :]
    inner_grad_ref[...] = (mixed_grad * input_ref[...].astype(jnp.float32)).astype(jnp.bfloat16)
    input_grad_ref[...] = (mixed_grad * inner_ref[...].astype(jnp.float32)).astype(jnp.bfloat16)
    for k in range(experts):
        expert = seat.ahead(offs[k])
        landed(c_ref.at[1 - seat.half, expert], us.at[k], ur.at[k])
        for swap in range(2):
            if k == 0 and swap == 0:
                continue
            half = seat.half if swap == 0 else 1 - seat.half
            landed(g_ref.at[half, expert], gs.at[k, swap], gr.at[k, swap])
            add_out(half, expert)
    for copy in started:
        copy.wait_send()


def vmem(count):
    return [pl.BlockSpec(memory_space=pltpu.VMEM)] * count


def hbm(count):
    return [pl.BlockSpec(memory_space=pltpu.HBM)] * count


def sems(*shape):
    return pltpu.SemaphoreType.DMA(shape)


def dispatch(routes, route_weights, stream, cotangent, inner, given, capacity, experts, tp_count):
    pairs = tp_count // 2
    tokens, model_width = stream.shape
    width = model_width // tp_count
    border = min(16, tokens)
    shape = jax.ShapeDtypeStruct((2, experts, capacity, model_width), jnp.bfloat16)
    halo = (border, inner.shape[1])
    flat, rowed = (2, experts), (2, experts, pairs)
    cored = (2, experts, 2 * pairs)
    return pl.pallas_call(
        functools.partial(dispatch_kernel, experts, pairs),
        out_shape=(
            shape,
            shape,
            jax.ShapeDtypeStruct((experts * capacity, tokens), jnp.bfloat16),
            jax.ShapeDtypeStruct(halo, jnp.float32),
        ),
        in_specs=hbm(6),
        out_specs=tuple(vmem(4)),
        scratch_shapes=[
            pltpu.VMEM((2, experts, capacity, width), jnp.bfloat16),
            pltpu.VMEM(halo, jnp.float32),
            pltpu.VMEM((2, tokens), jnp.int32),
            pltpu.VMEM((2, tokens), jnp.float32),
            pltpu.VMEM((2, tokens, width), jnp.bfloat16),
            pltpu.VMEM((2,) + halo, jnp.bfloat16),
        ]
        + [
            sems(*s)
            for s in (
                flat, flat, flat, flat, rowed, rowed, rowed, rowed, cored, cored,
                (2,), (1,), (1,), (6,),
            )
        ],
        compiler_params=pltpu.CompilerParams(
            collective_id=0, has_side_effects=True, vmem_limit_bytes=12 * 1024 * 1024
        ),
    )(routes.T, route_weights.T, stream, cotangent, inner, given)


def give_back(part, select, cotangent, conv_out, conv_sum, outer, inner, given, taps,
              out_weight, rows, routed, hidden, gate_delta, up_delta, experts, tp_count):
    pairs = tp_count // 2
    _, _, capacity, model_width = part.shape
    tokens, channels = conv_out.shape
    width = model_width // tp_count
    slice_width = model_width // (2 * experts)
    border = min(8, tokens)
    most = max(pairs, 2 * (pairs - 1))
    late = max(pairs - 1, 1)
    bf16 = jnp.bfloat16
    units = hidden.shape[1]
    gate_shape = jax.ShapeDtypeStruct((model_width, units), bf16)
    own_channels = jax.ShapeDtypeStruct((tokens, channels), bf16)
    return pl.pallas_call(
        functools.partial(return_kernel, experts, pairs),
        out_shape=(
            gate_shape,
            gate_shape,
            jax.ShapeDtypeStruct((units, model_width), bf16),
            jax.ShapeDtypeStruct((slice_width, channels), jnp.float32),
            own_channels,
            own_channels,
            own_channels,
        ),
        in_specs=vmem(2) + hbm(1) + vmem(6) + hbm(1) + vmem(5),
        out_specs=tuple(vmem(7)),
        scratch_shapes=[
            pltpu.VMEM((tokens, width), bf16),
            pltpu.VMEM((model_width, channels), bf16),
            pltpu.VMEM((tokens, model_width), bf16),
            pltpu.VMEM((2, experts, tokens, slice_width), bf16),
            pltpu.VMEM((2, experts, tokens, channels), bf16),
            pltpu.VMEM((tokens + border, channels), jnp.float32),
            pltpu.VMEM((border, channels), jnp.float32),
            pltpu.VMEM((2, pairs, experts, capacity, width), bf16),
            pltpu.VMEM((2, pairs, experts, capacity, width), bf16),
            pltpu.VMEM((experts, most, capacity, width), bf16),
            pltpu.VMEM((experts, max(pairs, 2), capacity, width), bf16),
            pltpu.VMEM((experts, late, capacity, width), bf16),
            pltpu.VMEM((experts, capacity, width), bf16),
            pltpu.VMEM((experts * capacity, width), bf16),
        ]
        + [
            sems(*s)
            for shape in (
                (2, pairs, experts), (experts, most), (experts, late), (experts,),
                (2 * pairs,), (experts, 2), (experts,), (experts,), (1,),
            )
            for s in (shape, shape)
        ]
        + [sems(4)],
        compiler_params=pltpu.CompilerParams(
            collective_id=1, has_side_effects=True, vmem_limit_bytes=18 * 1024 * 1024
        ),
    )(
        part, select, cotangent, conv_out, conv_sum, outer, inner, given, taps, out_weight,
        rows, routed, hidden, gate_delta, up_delta,
    )


def per_device(
    cotangent,
    stream,
    routes,
    route_weights,
    gate_weight,
    up_weight,
    down_weight,
    outer_gate,
    inner_gate,
    conv_input,
    conv_taps,
    out_weight,
):
    groups = lax.axis_size("sp")
    tp_count = lax.axis_size("tp")
    experts = groups // 2
    tok_rows = stream.shape[0]
    model_width = stream.shape[1]
    capacity = 3 * tok_rows // experts
    slot_total = experts * capacity
    contract_first = (((0,), (0,)), ((), ()))
    contract_last = (((1,), (1,)), ((), ()))
    block_width = model_width // tp_count
    slots = groups * capacity
    direct = tp_count % 2 == 0 and capacity % 16 == 0 and block_width % 128 == 0
    taps = conv_taps.astype(jnp.float32)
    outer_f = outer_gate.astype(jnp.float32)
    inner_f = inner_gate.astype(jnp.float32)
    input_f = conv_input.astype(jnp.float32)
    mixed = inner_f * input_f
    if direct:
        routed_rows, routed_cot, select, early = dispatch(
            routes, route_weights, stream, cotangent, inner_gate, conv_input,
            capacity, experts, tp_count,
        )
        routed_rows = routed_rows.reshape(slots, model_width)
        routed_cot = routed_cot.reshape(slots, model_width)
        earlier = jnp.where(lax.axis_index("sp") == 0, 0.0, early[-2:])
    else:
        flat_routes = routes.reshape(-1)
        choose = (flat_routes[:, None] == jnp.arange(experts, dtype=jnp.int32)[None, :]).astype(
            jnp.int32
        )
        before = jnp.cumsum(choose, axis=0) - choose
        slot_place = flat_routes * capacity + jnp.sum(before * choose, axis=1)
        slot_table = (jnp.arange(slot_total, dtype=jnp.int32)[:, None] == slot_place[None, :]).astype(
            jnp.float32
        )
        select = jnp.sum(slot_table.reshape(slot_total, tok_rows, 2), axis=2).astype(jnp.bfloat16)
        slot_weight = jnp.sum(slot_table * route_weights.reshape(-1)[None, :], axis=1)
        offset = lax.axis_index("tp") * block_width
        rows_part = lax.dynamic_slice_in_dim(stream, offset, block_width, 1)
        cot_part = lax.dynamic_slice_in_dim(cotangent, offset, block_width, 1)
        sent_rows = jnp.dot(select, rows_part, preferred_element_type=jnp.float32).astype(jnp.bfloat16)
        sent_cot = (
            jnp.dot(select, cot_part, preferred_element_type=jnp.float32) * slot_weight[:, None]
        ).astype(jnp.bfloat16)
        sent_rows = jnp.repeat(sent_rows.reshape(experts, capacity, -1), 2, axis=0)
        sent_cot = jnp.repeat(sent_cot.reshape(experts, capacity, -1), 2, axis=0)
        recv_rows, recv_cot = (
            lax.all_to_all(sent_rows, "sp", split_axis=0, concat_axis=0, tiled=True),
            lax.all_to_all(sent_cot, "sp", split_axis=0, concat_axis=0, tiled=True),
        )
        recv_rows, recv_cot = (
            lax.all_gather(recv_rows, "tp", axis=2, tiled=True),
            lax.all_gather(recv_cot, "tp", axis=2, tiled=True),
        )
        routed_rows = recv_rows.reshape(slots, model_width)
        routed_cot = recv_cot.reshape(slots, model_width)
        earlier = from_behind(mixed[-2:], "sp", 1)
    gate_local = gate_weight[0]
    up_local = up_weight[0]
    down_local = down_weight[0]
    gate_pre = jnp.dot(routed_rows, gate_local, preferred_element_type=jnp.float32)
    up_pre = jnp.dot(routed_rows, up_local, preferred_element_type=jnp.float32)
    hidden_grad = lax.dot_general(
        routed_cot, down_local, contract_last, preferred_element_type=jnp.float32
    )
    sigma = jax.nn.sigmoid(gate_pre)
    silu_gate = gate_pre * sigma
    hidden = (silu_gate * up_pre).astype(jnp.bfloat16)
    up_delta = (hidden_grad * silu_gate).astype(jnp.bfloat16)
    gate_delta = (hidden_grad * up_pre * sigma * (1.0 + gate_pre * (1.0 - sigma))).astype(
        jnp.bfloat16
    )
    row_partial = lax.dot_general(
        gate_delta, gate_local, contract_last, preferred_element_type=jnp.float32
    )
    row_partial = row_partial + lax.dot_general(
        up_delta, up_local, contract_last, preferred_element_type=jnp.float32
    )
    padded = jnp.concatenate([earlier, mixed], axis=0)
    conv_sum = taps[0] * padded[:-2] + taps[1] * padded[1:-1] + taps[2] * padded[2:]
    conv_out = (outer_f * conv_sum).astype(jnp.bfloat16)
    if direct:
        gate_grad, up_grad, down_grad, out_grad, outer_grad, inner_grad, input_grad = give_back(
            row_partial.astype(jnp.bfloat16).reshape(2, experts, capacity, model_width),
            select,
            cotangent,
            conv_out,
            conv_sum,
            outer_gate,
            inner_gate,
            conv_input,
            taps,
            out_weight,
            routed_rows,
            routed_cot,
            hidden,
            gate_delta,
            up_delta,
            experts,
            tp_count,
        )
        gate_grad, up_grad, down_grad = gate_grad[None], up_grad[None], down_grad[None]
    else:
        gate_grad = lax.dot_general(
            routed_rows, gate_delta, contract_first, preferred_element_type=jnp.float32
        ).astype(jnp.bfloat16)[None]
        up_grad = lax.dot_general(
            routed_rows, up_delta, contract_first, preferred_element_type=jnp.float32
        ).astype(jnp.bfloat16)[None]
        down_grad = lax.dot_general(
            hidden, routed_cot, contract_first, preferred_element_type=jnp.float32
        ).astype(jnp.bfloat16)[None]
        half_sums = lax.psum_scatter(
            row_partial.astype(jnp.bfloat16), "tp", scatter_dimension=1, tiled=True
        ).astype(jnp.float32)
        block_width = half_sums.shape[1]
        half_grad = half_sums.reshape(groups, capacity, block_width).astype(jnp.bfloat16)
        returned = lax.all_to_all(half_grad, "sp", split_axis=0, concat_axis=0, tiled=True)
        returned = returned.reshape(experts, 2, capacity, block_width)
        select_three = select.reshape(experts, capacity, tok_rows)
        moe_part = jnp.einsum(
            "ecr,emcd->rd", select_three, returned, preferred_element_type=jnp.float32
        ).astype(jnp.bfloat16)
        moe_grad = lax.all_gather(moe_part, "tp", axis=1, tiled=True)
        stream_grad = (cotangent.astype(jnp.float32) + moe_grad.astype(jnp.float32)).astype(
            jnp.bfloat16
        )
        out_grad = lax.psum_scatter(
            lax.dot_general(
                stream_grad, conv_out, contract_first, preferred_element_type=jnp.float32
            ).astype(jnp.bfloat16),
            "sp",
            scatter_dimension=0,
            tiled=True,
        ).astype(jnp.float32)
        conv_grad = jnp.dot(stream_grad, out_weight, preferred_element_type=jnp.float32)
        outer_grad = (conv_grad * conv_sum).astype(jnp.bfloat16)
        scaled = conv_grad * outer_f
        later = from_behind(scaled[:2], "sp", -1)
        extended = jnp.concatenate([scaled, later], axis=0)
        mixed_grad = taps[2] * extended[:-2] + taps[1] * extended[1:-1] + taps[0] * extended[2:]
        inner_grad = (mixed_grad * input_f).astype(jnp.bfloat16)
        input_grad = (mixed_grad * inner_f).astype(jnp.bfloat16)
    return (gate_grad, up_grad, down_grad, out_grad, outer_grad, inner_grad, input_grad)


def solution(mesh):
    placed = (
        P("sp", None),
        P("sp", None),
        P("sp", None),
        P("sp", None),
        P("sp", None, "tp"),
        P("sp", None, "tp"),
        P("sp", "tp", None),
        P("sp", "tp"),
        P("sp", "tp"),
        P("sp", "tp"),
        P(None, "tp"),
        P(None, "tp"),
    )
    return jax.shard_map(
        per_device,
        mesh=mesh,
        in_specs=placed,
        out_specs=(
            P("sp", None, "tp"),
            P("sp", None, "tp"),
            P("sp", "tp", None),
            P("sp", "tp"),
            P("sp", "tp"),
            P("sp", "tp"),
            P("sp", "tp"),
        ),
        check_vma=False,
    )
```
